32 devices in a mesh: sp: 16 (over z, y, x), tp: 2 (over core).
Axes of the slice: x: 2, y: 2, z: 4, core: 2. Of those that a mesh axis runs over, the one named last changes fastest.
Arguments:
- latent: bfloat16 [12288, 2048], P(('sp', 'tp')), may hold values from -6 to 6
- condition: float32 [2048], P('sp'), may hold values from -6 to 6
- context_condition: float32 [2048], P('sp'), may hold values from -6 to 6
- context: bfloat16 [1024, 2048], P('sp'), may hold values from -6 to 6
- norm_gain: float32 [2048], replicated, may hold values from 0.1 to 1.9
- shift_weight: bfloat16 [2048, 2048], P('sp', 'tp'), may hold values from -0.1875 to 0.1875
- scale_weight: bfloat16 [2048, 2048], P('sp', 'tp'), may hold values from -0.1875 to 0.1875
- gate_weight: bfloat16 [2048, 2048], P('sp', 'tp'), may hold values from -0.1875 to 0.1875
- query_weight: bfloat16 [2048, 2048], P(None, 'tp'), may hold values from -2 to 2
- key_matrix: bfloat16 [2048, 1024], P(None, 'tp'), may hold values from -2 to 2
- value_matrix: bfloat16 [2048, 1024], P(None, 'tp'), may hold values from -0.125 to 0.125
- sink_logit_head: float32 [16], P('tp'), may hold values from 6 to 10
- out_weight: bfloat16 [2048, 2048], P('tp'), may hold values from -0.125 to 0.125
Outputs:
- updated: bfloat16 [12288, 2048], P(('sp', 'tp'))
The draws below stay inside these ranges and needn't reach their ends.
All inputs are finite; a program needn't handle non-finite values.
Results may differ from the reference program's by a relative error of at most 0.012.
The reference program's roundings to bfloat16 on the way count: a program that leaves them out, or rounds other values in their place, can miss the bound.
Values may be sent and summed in bfloat16 or wider, within the bound.
A program may use at most 128 MiB of HBM per device.

```python
import jax
import jax.numpy as jnp
from jax import lax

MODEL_DIM = 2048
QUERY_HEADS = 16
KEY_VALUE_HEADS = 8
HEAD_DIM = 128
WINDOW_REACH = 128
GRID_W = 64
CTX = 1024
TOKENS = 12288
N_TP = 2


def query_shared_group(key):
    return jax.random.normal(jax.random.fold_in(key, 101), (MODEL_DIM, QUERY_HEADS * HEAD_DIM), jnp.float32) * MODEL_DIM ** (-0.5)


def draw_query_weight(key, part):
    return query_shared_group(key).astype(jnp.bfloat16)


def draw_key_matrix(key, part):
    sampled_weights = jax.random.normal(jax.random.fold_in(key, 202), (MODEL_DIM, KEY_VALUE_HEADS * HEAD_DIM), jnp.float32) * MODEL_DIM ** (-0.5)
    return sampled_weights.astype(jnp.bfloat16)


def raised(drawn, stream_key, source, target, shards_of, factor):
    owner, partner = [(jnp.arange(drawn.shape[dim]) // (drawn.shape[dim] // shards_of)).reshape([-1 if axis == dim else 1 for axis in range(drawn.ndim)]) for dim in (source, target)]
    chosen = jax.random.permutation(stream_key, shards_of)[partner]
    strong = (owner == chosen) | (owner == (partner + shards_of // 2) % shards_of)
    return jnp.where(strong, factor * drawn, drawn)


def level_of(stream_key, dims, cuts, low, top_value):
    def one(axis_at, parts):
        steps = jax.random.uniform(jax.random.fold_in(jax.random.fold_in(stream_key, 6), axis_at), (parts,), jnp.float32, low / len(cuts), top_value / len(cuts))
        return jnp.repeat(jnp.exp(steps), dims[axis_at] // parts).reshape((-1,) + (1,) * (len(dims) - axis_at - 1))

    gain = one(*cuts[0])
    for cut in cuts[1:]:
        gain = gain * one(*cut)
    return gain


def normal_values(key, dims, spread, most, cuts=(), kind=jnp.bfloat16):
    drawn = spread * jax.random.normal(key, dims, jnp.float32)
    if cuts:
        drawn = drawn * level_of(key, dims, cuts, -0.22, 0.18)
    return jnp.clip(drawn, -most, most).astype(kind)


def heavy_noise(stream_key, extent, scale, most, cuts, heavy, kind=jnp.bfloat16):
    values = scale * jax.random.normal(stream_key, extent, jnp.float32)
    if cuts:
        values = values * level_of(stream_key, extent, cuts, -0.22, 0.18)
    return jnp.clip(raised(values, jax.random.fold_in(stream_key, 3), *heavy), -most, most).astype(kind)


def setup_inputs(seed: int = 0) -> dict:
    key_list = jax.random.split(jax.random.key(seed), 14)
    latent = normal_values(key_list[0], (TOKENS, MODEL_DIM), 1.0, 6.0, ((0, 32),))
    condition = normal_values(key_list[1], (MODEL_DIM,), 1.0, 6.0, ((0, 16),), jnp.float32)
    context_condition = normal_values(key_list[2], (MODEL_DIM,), 1.0, 6.0, ((0, 16),), jnp.float32)
    context = normal_values(key_list[3], (CTX, MODEL_DIM), 1.0, 6.0, ((0, 16),))
    norm_gain = jnp.clip(1.0 + 0.18 * jax.random.normal(key_list[4], (MODEL_DIM,), jnp.float32), 0.1, 1.9)
    shift_weight = heavy_noise(key_list[5], (MODEL_DIM, MODEL_DIM), MODEL_DIM ** -0.5, 0.1875, ((0, 16), (1, 2)), (0, 1, 16, 2.0))
    scale_weight = heavy_noise(key_list[6], (MODEL_DIM, MODEL_DIM), MODEL_DIM ** -0.5, 0.1875, ((0, 16), (1, 2)), (0, 1, 16, 2.0))
    gate_weight = heavy_noise(key_list[7], (MODEL_DIM, MODEL_DIM), MODEL_DIM ** -0.5, 0.1875, ((0, 16), (1, 2)), (0, 1, 16, 2.0))
    query_weight = draw_query_weight(jax.random.fold_in(key_list[13], 71), 0)
    key_matrix = draw_key_matrix(jax.random.fold_in(key_list[13], 71), 0)
    value_matrix = normal_values(key_list[10], (MODEL_DIM, KEY_VALUE_HEADS * HEAD_DIM), MODEL_DIM ** -0.5, 0.125, ((1, 2),))
    sink_logit_head = jnp.clip(6.0 + 4.0 * jax.random.uniform(key_list[11], (QUERY_HEADS,), jnp.float32) ** level_of(key_list[11], (QUERY_HEADS,), ((0, 2),), -0.2, 0.2), 6.0, 10.0)
    out_weight = normal_values(key_list[12], (QUERY_HEADS * HEAD_DIM, MODEL_DIM), (QUERY_HEADS * HEAD_DIM) ** -0.5, 0.125, ((0, 2),))
    return {"latent": latent, "condition": condition, "context_condition": context_condition, "context": context, "norm_gain": norm_gain, "shift_weight": shift_weight, "scale_weight": scale_weight, "gate_weight": gate_weight, "query_weight": query_weight, "key_matrix": key_matrix, "value_matrix": value_matrix, "sink_logit_head": sink_logit_head, "out_weight": out_weight}


NORM_EPS = 1e-05
MASKED_SCORE = -1e+30

def rotate(vectors, position):
    quarter = HEAD_DIM // 4
    grid_row = (position // GRID_W).astype(jnp.float32)
    grid_col = (position % GRID_W).astype(jnp.float32)
    inv_freq = 10000.0 ** (-jnp.arange(0, HEAD_DIM // 2, 2, dtype=jnp.float32) / (HEAD_DIM // 2))
    angles = jnp.concatenate([grid_row[:, None] * inv_freq, grid_col[:, None] * inv_freq], axis=-1)
    cosine_table = jnp.cos(angles).reshape(-1, 1, 2, quarter)
    sine_table = jnp.sin(angles).reshape(-1, 1, 2, quarter)
    pieces = vectors.reshape(vectors.shape[0], vectors.shape[1], 2, 2, quarter)
    first_half = pieces[..., 0, :]
    second_half = pieces[..., 1, :]
    turned = jnp.stack([first_half * cosine_table - second_half * sine_table, first_half * sine_table + second_half * cosine_table], axis=-2)
    return turned.reshape(vectors.shape)

def modulation(vector, weight):
    active = jax.nn.silu(vector).astype(jnp.bfloat16)
    return jnp.dot(active[None, :], weight, preferred_element_type=jnp.float32)[0]

def modulated_norm(rows_in, norm_gain, shift, scale):
    floats = rows_in.astype(jnp.float32)
    normed = floats * lax.rsqrt(lax.optimization_barrier(jnp.mean(floats * floats, axis=-1, keepdims=True)) + NORM_EPS) * norm_gain
    return (normed * (1.0 + scale) + shift).astype(jnp.bfloat16)

def attend(queries, joined_keys, joined_values, context_key_rows, context_value_rows, sink_logit_head):
    latent_token_count = queries.shape[0]
    blocks = latent_token_count // WINDOW_REACH
    queries_per_group = QUERY_HEADS // KEY_VALUE_HEADS
    padding = ((WINDOW_REACH, WINDOW_REACH), (0, 0), (0, 0))
    keys_pad = jnp.pad(joined_keys, padding)
    values_pad = jnp.pad(joined_values, padding)
    ctx_key_f = context_key_rows.astype(jnp.float32)
    ctx_value_f = context_value_rows.astype(jnp.float32)
    factor = HEAD_DIM ** (-0.5)
    sink_logit_rows = sink_logit_head.reshape(KEY_VALUE_HEADS, queries_per_group, 1, 1)

    def one_block(block_index):
        begin_row = block_index * WINDOW_REACH
        query_row_block = lax.dynamic_slice_in_dim(queries, begin_row, WINDOW_REACH, 0)
        query_row_block = query_row_block.reshape(WINDOW_REACH, KEY_VALUE_HEADS, queries_per_group, HEAD_DIM).astype(jnp.float32)
        band_keys = lax.dynamic_slice_in_dim(keys_pad, begin_row, 3 * WINDOW_REACH, 0).astype(jnp.float32)
        band_values = lax.dynamic_slice_in_dim(values_pad, begin_row, 3 * WINDOW_REACH, 0).astype(jnp.float32)
        band_scores = jnp.einsum('qhgd,khd->hgqk', query_row_block, band_keys) * factor
        query_pos = begin_row + jnp.arange(WINDOW_REACH, dtype=jnp.int32)[:, None]
        key_pos = begin_row - WINDOW_REACH + jnp.arange(3 * WINDOW_REACH, dtype=jnp.int32)[None, :]
        allowed = (jnp.abs(key_pos - query_pos) <= WINDOW_REACH) & (key_pos >= 0) & (key_pos < latent_token_count)
        band_scores = jnp.where(allowed[None, None], band_scores, MASKED_SCORE)
        ctx_scores = jnp.einsum('qhgd,chd->hgqc', query_row_block, ctx_key_f) * factor
        maxima = jnp.maximum(jnp.maximum(lax.optimization_barrier(jnp.max(band_scores, axis=-1, keepdims=True)), lax.optimization_barrier(jnp.max(ctx_scores, axis=-1, keepdims=True))), sink_logit_rows)
        band_exp = jnp.exp(band_scores - maxima)
        ctx_exp = jnp.exp(ctx_scores - maxima)
        denominator = lax.optimization_barrier(jnp.sum(band_exp, axis=-1, keepdims=True)) + lax.optimization_barrier(jnp.sum(ctx_exp, axis=-1, keepdims=True)) + jnp.exp(sink_logit_rows - maxima)
        band_weights = (band_exp / denominator).astype(jnp.bfloat16).astype(jnp.float32)
        ctx_weights = (ctx_exp / denominator).astype(jnp.bfloat16).astype(jnp.float32)
        summed = jnp.einsum('hgqk,khd->qhgd', band_weights, band_values) + jnp.einsum('hgqc,chd->qhgd', ctx_weights, ctx_value_f)
        return summed.astype(jnp.bfloat16).reshape(WINDOW_REACH, QUERY_HEADS * HEAD_DIM)
    blocks_out = lax.map(one_block, jnp.arange(blocks, dtype=jnp.int32))
    return blocks_out.reshape(latent_token_count, QUERY_HEADS * HEAD_DIM)

def reference(latent, condition, context_condition, context, norm_gain, shift_weight, scale_weight, gate_weight, query_weight, key_matrix, value_matrix, sink_logit_head, out_weight):
    shift = modulation(condition, shift_weight)
    scale = modulation(condition, scale_weight)
    gate = modulation(condition, gate_weight)
    ctx_shift = modulation(context_condition, shift_weight)
    ctx_scale = modulation(context_condition, scale_weight)
    hidden_state = modulated_norm(latent, norm_gain, shift, scale)
    ctx_hidden = modulated_norm(context, norm_gain, ctx_shift, ctx_scale)
    latent_token_count = latent.shape[0]
    position = jnp.arange(latent_token_count, dtype=jnp.int32)
    queries = jnp.dot(hidden_state, query_weight, preferred_element_type=jnp.float32).reshape(latent_token_count, QUERY_HEADS, HEAD_DIM)
    queries = rotate(queries, position).astype(jnp.bfloat16)
    joined_keys = jnp.dot(hidden_state, key_matrix, preferred_element_type=jnp.float32).reshape(latent_token_count, KEY_VALUE_HEADS, HEAD_DIM)
    joined_keys = rotate(joined_keys, position).astype(jnp.bfloat16)
    joined_values = jnp.dot(hidden_state, value_matrix, preferred_element_type=jnp.float32).astype(jnp.bfloat16)
    joined_values = joined_values.reshape(latent_token_count, KEY_VALUE_HEADS, HEAD_DIM)
    context_key_rows = jnp.dot(ctx_hidden, key_matrix, preferred_element_type=jnp.float32).astype(jnp.bfloat16)
    context_value_rows = jnp.dot(ctx_hidden, value_matrix, preferred_element_type=jnp.float32).astype(jnp.bfloat16)
    context_key_rows = context_key_rows.reshape(-1, KEY_VALUE_HEADS, HEAD_DIM)
    context_value_rows = context_value_rows.reshape(-1, KEY_VALUE_HEADS, HEAD_DIM)
    attended = attend(queries, joined_keys, joined_values, context_key_rows, context_value_rows, sink_logit_head)
    group_width = QUERY_HEADS * HEAD_DIM // N_TP
    mixed_sum = jnp.zeros((latent_token_count, latent.shape[1]), jnp.float32)
    for member in range(N_TP):
        partial_value = jnp.dot(attended[:, member * group_width:(member + 1) * group_width], out_weight[member * group_width:(member + 1) * group_width], preferred_element_type=jnp.float32)
        rounded = lax.optimization_barrier(partial_value.astype(jnp.bfloat16))
        mixed_sum = mixed_sum + rounded.astype(jnp.float32)
    return (latent.astype(jnp.float32) + gate * mixed_sum).astype(jnp.bfloat16)
```

```python
import functools

import jax
import jax.numpy as jnp
import numpy as np
from jax import lax
from jax.experimental import pallas as pl
from jax.experimental.pallas import tpu as pltpu
from jax.sharding import PartitionSpec as P

QUERY_HEADS = 16
KEY_VALUE_HEADS = 8
HEAD_DIM = 128
WINDOW_REACH = 128
GRID_W = 64
NORM_EPS = 1e-05
MASKED_SCORE = -1e30
LANES = 128
QUAD = 4
MESH = pl.DeviceIdType.MESH
F32 = jnp.float32
BF16 = jnp.bfloat16


def tile_of(extent, most):
    tile = min(extent, most)
    while extent % tile:
        tile -= LANES
    return tile


def block_kernel(
    n_sp,
    n_tp,
    cond_ref,
    ctx_cond_ref,
    gain_ref,
    row_cos,
    row_sin,
    col_cos,
    col_sin,
    sink_ref,
    latent_hbm,
    context_hbm,
    shift_hbm,
    scale_hbm,
    gate_hbm,
    wq_hbm,
    wk_hbm,
    wv_hbm,
    wo_hbm,
    out_ref,
    latent,
    context,
    shift_w,
    scale_w,
    gate_w,
    wq,
    wk,
    wv,
    wo,
    part,
    gathered,
    full,
    mod,
    hidden,
    ctx_hidden,
    queries,
    kv,
    ctx_kv,
    attended,
    partial_out,
    partial_in,
    own_total,
    cos_ref,
    sin_ref,
    halo_raw,
    load_sem,
    rs_send,
    rs_recv,
    ag_send,
    ag_recv,
    hid_send,
    hid_recv,
    ctx_send,
    ctx_recv,
    halo_send,
    halo_recv,
    raw_send,
    raw_recv,
    edge_send,
    edge_recv,
    out_send,
    out_recv,
):
    sp = lax.axis_index("sp")
    tp = lax.axis_index("tp")
    rows, width = latent.shape
    group_rows = rows * n_tp
    columns = shift_w.shape[1]
    chunks = columns // LANES
    per = part.shape[1]
    query_width = wq.shape[1]
    pair = wk.shape[1]
    kv_local = pair // HEAD_DIM
    per_group = query_width // pair
    ctx_rows = context.shape[0]

    loads = [
        pltpu.make_async_copy(src, dst, load_sem.at[i])
        for i, (src, dst) in enumerate(
            [
                (shift_hbm, shift_w),
                (scale_hbm, scale_w),
                (gate_hbm, gate_w),
                (context_hbm, context),
                (latent_hbm, latent),
                (wk_hbm, wk),
                (wv_hbm, wv),
                (wq_hbm, wq),
                (wo_hbm, wo),
            ]
        )
    ]
    for load in loads:
        load.start()

    barrier = pltpu.get_barrier_semaphore()

    everyone = n_sp * n_tp
    me = sp * n_tp + tp

    def other(d):
        at = lax.rem(me + d, everyone)
        return at // n_tp, lax.rem(at, n_tp)

    def greet(d, carry):
        peer_sp, peer_tp = other(d)
        pl.semaphore_signal(
            barrier, inc=1, device_id={"sp": peer_sp, "tp": peer_tp}, device_id_type=MESH
        )
        return carry

    lax.fori_loop(1, everyone, greet, 0)

    def silu(v):
        return v / (1.0 + jnp.exp(-v))

    depth = cond_ref.shape[1]
    row_id = lax.broadcasted_iota(jnp.int32, (16, depth), 0)
    active = jnp.where(
        row_id == 0,
        jnp.broadcast_to(silu(cond_ref[...]), (16, depth)),
        jnp.broadcast_to(silu(ctx_cond_ref[...]), (16, depth)),
    ).astype(BF16)
    part[...] = jnp.zeros_like(part)
    vector = 0
    for load, weight, count in zip(loads[:3], (shift_w, scale_w, gate_w), (2, 2, 1)):
        load.wait()
        product = jnp.dot(active, weight[...], preferred_element_type=F32)
        for v in range(count):
            for j in range(chunks):
                g = vector * chunks + j
                part[g // per, g % per : g % per + 1, :] = product[
                    v : v + 1, j * LANES : (j + 1) * LANES
                ]
            vector += 1

    pl.semaphore_wait(barrier, everyone - 1)

    def rs_copy(d):
        peer = lax.rem(sp + d, n_sp)
        return pltpu.make_async_remote_copy(
            src_ref=part.at[peer],
            dst_ref=gathered.at[sp],
            send_sem=rs_send.at[peer],
            recv_sem=rs_recv.at[sp],
            device_id={"sp": peer},
            device_id_type=MESH,
        )

    def rs_arrival(d):
        peer = lax.rem(sp + d, n_sp)
        return pltpu.make_async_remote_copy(
            src_ref=part.at[peer],
            dst_ref=gathered.at[peer],
            send_sem=rs_send.at[peer],
            recv_sem=rs_recv.at[peer],
            device_id={"sp": peer},
            device_id_type=MESH,
        )

    def loop(low, high, f):
        def step(i, carry):
            f(i)
            return carry

        lax.fori_loop(low, high, step, 0)

    raw_halo = rows >= WINDOW_REACH
    has_next, has_last = sp < n_sp - 1, sp > 0
    holds_last, holds_first = tp == n_tp - 1, tp == 0
    half_reach = WINDOW_REACH // 2

    def raw_copy(up, half):
        which = 0 if up else 1
        base = rows - WINDOW_REACH if up else 0
        return pltpu.make_async_remote_copy(
            src_ref=latent.at[pl.ds(base + half * half_reach, half_reach)],
            dst_ref=halo_raw.at[which, pl.ds(half * half_reach, half_reach)],
            send_sem=raw_send.at[which, half],
            recv_sem=raw_recv.at[which, half],
            device_id={"sp": lax.rem(sp + (1 if up else n_sp - 1), n_sp)},
            device_id_type=MESH,
        )

    def send_raw(half):
        if raw_halo:

            @pl.when(has_next & holds_last)
            def _():
                raw_copy(True, half).start()

            @pl.when(has_last & holds_first)
            def _():
                raw_copy(False, half).start()

    loop(1, n_sp, lambda d: rs_copy(d).start())
    gathered[sp] = part[sp]
    loads[4].wait()
    send_raw(0)

    strip = 32

    def scale_strip(i):
        at = pl.multiple_of(i * strip, strip)
        floats = latent[pl.ds(at, strip), :].astype(F32)
        inverse = lax.rsqrt(jnp.mean(floats * floats, axis=-1, keepdims=True) + NORM_EPS)
        own_total[pl.ds(at, strip), :] = floats * inverse

    loop(0, rows // strip, scale_strip)

    grid_rows = group_rows // GRID_W
    grid_pad = WINDOW_REACH // GRID_W
    in_row = lax.broadcasted_iota(jnp.int32, (GRID_W, HEAD_DIM), 1) < HEAD_DIM // 2

    def fill_angles(i):
        row = jnp.clip(sp * grid_rows - grid_pad + i, 0, n_sp * grid_rows - 1)
        at = pl.ds(pl.multiple_of(i * GRID_W, GRID_W), GRID_W)
        for target, by_row, by_col in ((cos_ref, row_cos, col_cos), (sin_ref, row_sin, col_sin)):
            spread = jnp.broadcast_to(by_row[pl.ds(row, 1), :], (GRID_W, HEAD_DIM))
            target[at, :] = jnp.where(in_row, spread, by_col[...])

    loop(0, grid_rows + 2 * grid_pad, fill_angles)
    loop(1, n_sp, lambda d: rs_arrival(d).wait_recv())
    full[tp, sp] = jnp.sum(gathered[...], axis=0)

    def ag_copy(d):
        peer_sp, peer_tp = other(d)
        return pltpu.make_async_remote_copy(
            src_ref=full.at[tp, sp],
            dst_ref=full.at[tp, sp],
            send_sem=ag_send.at[peer_tp, peer_sp],
            recv_sem=ag_recv.at[tp, sp],
            device_id={"sp": peer_sp, "tp": peer_tp},
            device_id_type=MESH,
        )

    def ag_arrival(d):
        peer_sp, peer_tp = other(d)
        return pltpu.make_async_remote_copy(
            src_ref=full.at[tp, sp],
            dst_ref=full.at[peer_tp, peer_sp],
            send_sem=ag_send.at[peer_tp, peer_sp],
            recv_sem=ag_recv.at[peer_tp, peer_sp],
            device_id={"sp": peer_sp, "tp": peer_tp},
            device_id_type=MESH,
        )

    loop(1, everyone, lambda d: ag_copy(d).start())
    send_raw(1)

    loop(1, everyone, lambda d: ag_arrival(d).wait_recv())

    for t in range(n_tp):
        for v in range(5):
            for j in range(chunks):
                g = v * chunks + j
                column = t * columns + j * LANES
                mod[v : v + 1, column : column + LANES] = full[t, g // per, g % per : g % per + 1, :]
    gain = gain_ref[...]
    mod[2:3, :] = gain * (1.0 + mod[2:3, :])
    mod[3:4, :] = gain * (1.0 + mod[3:4, :])

    def normed(block, shift_row, scale_row):
        floats = block.astype(F32)
        inverse = lax.rsqrt(jnp.mean(floats * floats, axis=-1, keepdims=True) + NORM_EPS)
        return (
            floats * inverse * mod[scale_row : scale_row + 1, :] + mod[shift_row : shift_row + 1, :]
        ).astype(BF16)

    for i in (3, 5, 6):
        loads[i].wait()
    ctx_hidden[...] = normed(context[...], 1, 3)
    tile = tile_of(pair, 512)

    def ctx_project(j):
        at = pl.multiple_of(j * tile, tile)
        ctx_kv[sp, :, pl.ds(at, tile)] = jnp.dot(
            ctx_hidden[...], wk[:, pl.ds(at, tile)], preferred_element_type=F32
        ).astype(BF16)
        ctx_kv[sp, :, pl.ds(pl.multiple_of(pair + at, tile), tile)] = jnp.dot(
            ctx_hidden[...], wv[:, pl.ds(at, tile)], preferred_element_type=F32
        ).astype(BF16)

    loop(0, pair // tile, ctx_project)

    lines = n_sp // QUAD
    line, corner = sp // QUAD, lax.rem(sp, QUAD)

    across = corner + 1 - 2 * lax.rem(corner, 2)
    beside = lax.rem(corner + 2, QUAD)
    opposite = QUAD - 1 - corner

    def ctx_copy(slot, peer, sem, half=None):
        cols = slice(None) if half is None else pl.ds(half * pair, pair)
        return pltpu.make_async_remote_copy(
            src_ref=ctx_kv.at[slot, :, cols],
            dst_ref=ctx_kv.at[slot, :, cols],
            send_sem=ctx_send.at[sem],
            recv_sem=ctx_recv.at[slot, half or 0],
            device_id={"sp": peer},
            device_id_type=MESH,
        )

    ctx_sends = []

    def send_ctx(slot, peer, half=None):
        copy = ctx_copy(slot, peer, len(ctx_sends), half)
        copy.start()
        ctx_sends.append(copy)

    def send_quad(slot):
        send_ctx(slot, line * QUAD + across)
        send_ctx(slot, line * QUAD + beside)

    for d in range(1, lines):
        send_ctx(sp, lax.rem(line + d, lines) * QUAD + corner)
    send_quad(sp)

    def line_base(d):
        return lax.rem(line + lines - d, lines) * QUAD

    def forward(d):
        slot = line_base(d) + corner
        ctx_copy(slot, sp, 0).wait_recv()
        send_quad(slot)

    def relay(d):
        ctx_copy(line_base(d) + across, sp, 0).wait_recv()
        send_ctx(line_base(d) + across, line * QUAD + beside, 0)
        ctx_copy(line_base(d) + beside, sp, 0).wait_recv()
        send_ctx(line_base(d) + beside, line * QUAD + across, 1)

    def serve(step):
        if step < lines:
            if step + 1 < lines:
                forward(step + 1)
            relay(step)

    own_start = pl.multiple_of(WINDOW_REACH + tp * rows, strip)

    def norm_strip(i):
        at = pl.multiple_of(i * strip, strip)
        hidden[pl.ds(pl.multiple_of(own_start + at, strip), strip), :] = (
            own_total[pl.ds(at, strip), :] * mod[2:3, :] + mod[0:1, :]
        ).astype(BF16)

    loop(0, rows // strip, norm_strip)

    def hid_copy(d, mine):
        peer = lax.rem(tp + d, n_tp)
        slot = tp if mine else peer
        at = pl.multiple_of(WINDOW_REACH + slot * rows, strip)
        mine_at = pl.multiple_of(WINDOW_REACH + tp * rows, strip)
        return pltpu.make_async_remote_copy(
            src_ref=hidden.at[pl.ds(mine_at, rows)],
            dst_ref=hidden.at[pl.ds(at, rows)],
            send_sem=hid_send.at[peer],
            recv_sem=hid_recv.at[slot],
            device_id={"tp": peer},
            device_id_type=MESH,
        )

    loop(1, n_tp, lambda d: hid_copy(d, True).start())

    def edge_copy(low, d, mine):
        owner = n_tp - 1 if low else 0
        peer = lax.rem(tp + d, n_tp) if mine else tp
        which = 0 if low else 1
        region = pl.ds(0 if low else WINDOW_REACH + group_rows, WINDOW_REACH)
        return pltpu.make_async_remote_copy(
            src_ref=hidden.at[region],
            dst_ref=hidden.at[region],
            send_sem=edge_send.at[which, peer],
            recv_sem=edge_recv.at[which],
            device_id={"tp": peer},
            device_id_type=MESH,
        )

    def receive_edge(low):
        which = 0 if low else 1
        base = 0 if low else WINDOW_REACH + group_rows
        raw_copy(low, 0).wait_recv()
        raw_copy(low, 1).wait_recv()

        def one(i):
            at = pl.multiple_of(i * strip, strip)
            hidden[pl.ds(pl.multiple_of(base + at, strip), strip), :] = normed(
                halo_raw[which, pl.ds(at, strip), :], 0, 2
            )

        loop(0, WINDOW_REACH // strip, one)
        loop(1, n_tp, lambda d: edge_copy(low, d, True).start())

    quarter = HEAD_DIM // 4
    def turned(values, cosine, sine):
        pieces = []
        lane = lax.broadcasted_iota(jnp.int32, cosine.shape, 1)
        low_half = lax.rem(lane, 2 * quarter) < quarter
        for h in range(values.shape[1] // HEAD_DIM):
            u = values[:, h * HEAD_DIM : (h + 1) * HEAD_DIM]
            other = jnp.where(
                low_half, pltpu.roll(u, HEAD_DIM - quarter, 1), pltpu.roll(u, quarter, 1)
            )
            pieces.append(u * cosine + other * sine)
        return jnp.concatenate(pieces, axis=1).astype(BF16)

    def project_kv(start, count):
        source = pl.ds(pl.multiple_of(start, strip), count)

        def one(j):
            col = pl.multiple_of(j * tile, tile)
            keys = jnp.dot(hidden[source, :], wk[:, pl.ds(col, tile)], preferred_element_type=F32)
            kv[source, pl.ds(col, tile)] = turned(keys, cos_ref[source, :], sin_ref[source, :])
            values = jnp.dot(hidden[source, :], wv[:, pl.ds(col, tile)], preferred_element_type=F32)
            kv[source, pl.ds(pl.multiple_of(pair + col, tile), tile)] = values.astype(BF16)

        loop(0, pair // tile, one)

    def project_q(slot):
        target = pl.ds(pl.multiple_of(slot * rows, strip), rows)
        source = pl.ds(pl.multiple_of(WINDOW_REACH + slot * rows, strip), rows)
        q_tile = tile_of(query_width, 512)

        def one(j):
            col = pl.multiple_of(j * q_tile, q_tile)
            q = jnp.dot(hidden[source, :], wq[:, pl.ds(col, q_tile)], preferred_element_type=F32)
            queries[target, pl.ds(col, q_tile)] = turned(
                q * factor, cos_ref[source, :], sin_ref[source, :]
            )

        loop(0, query_width // q_tile, one)

    log2e = 1.4426950408889634
    factor = HEAD_DIM ** (-0.5) * log2e
    project_kv(WINDOW_REACH + tp * rows, rows)
    serve(0)
    loop(1, n_tp, lambda d: hid_copy(d, False).wait_recv())
    loop(1, n_tp, lambda d: project_kv(WINDOW_REACH + lax.rem(tp + d, n_tp) * rows, rows))
    serve(1)

    def halo_copy(up):
        source = group_rows if up else WINDOW_REACH
        target = 0 if up else group_rows + WINDOW_REACH
        which = 0 if up else 1
        return pltpu.make_async_remote_copy(
            src_ref=kv.at[pl.ds(source, WINDOW_REACH)],
            dst_ref=kv.at[pl.ds(target, WINDOW_REACH)],
            send_sem=halo_send.at[which],
            recv_sem=halo_recv.at[which],
            device_id={"sp": lax.rem(sp + (1 if up else n_sp - 1), n_sp)},
            device_id_type=MESH,
        )

    if not raw_halo:

        @pl.when(has_next)
        def _():
            halo_copy(True).start()

        @pl.when(has_last)
        def _():
            halo_copy(False).start()

        @pl.when(jnp.logical_not(has_last))
        def _():
            kv[0:WINDOW_REACH, :] = jnp.zeros((WINDOW_REACH, 2 * pair), BF16)

        @pl.when(jnp.logical_not(has_next))
        def _():
            kv[group_rows + WINDOW_REACH :, :] = jnp.zeros((WINDOW_REACH, 2 * pair), BF16)

    loads[7].wait()
    project_q(tp)
    serve(2)
    loop(1, n_tp, lambda d: project_q(lax.rem(tp + d, n_tp)))
    if raw_halo:

        @pl.when(has_last & holds_last)
        def _():
            receive_edge(True)

        @pl.when(has_next & holds_first)
        def _():
            receive_edge(False)

        @pl.when(jnp.logical_not(has_last))
        def _():
            hidden[0:WINDOW_REACH, :] = jnp.zeros((WINDOW_REACH, width), BF16)

        @pl.when(jnp.logical_not(has_next))
        def _():
            hidden[WINDOW_REACH + group_rows :, :] = jnp.zeros((WINDOW_REACH, width), BF16)

    for step in range(3, lines):
        serve(step)
    if raw_halo:

        @pl.when(has_last & jnp.logical_not(holds_last))
        def _():
            edge_copy(True, 0, False).wait_recv()

        @pl.when(has_next & jnp.logical_not(holds_first))
        def _():
            edge_copy(False, 0, False).wait_recv()

        project_kv(0, WINDOW_REACH)
        project_kv(WINDOW_REACH + group_rows, WINDOW_REACH)
    else:

        @pl.when(has_last)
        def _():
            halo_copy(True).wait_recv()

        @pl.when(has_next)
        def _():
            halo_copy(False).wait_recv()

    def opposite_arrivals(i):
        slot = i * QUAD + opposite
        ctx_copy(slot, sp, 0, 0).wait_recv()
        ctx_copy(slot, sp, 0, 1).wait_recv()

    loop(0, lines, opposite_arrivals)

    span = 3 * WINDOW_REACH
    stacked = per_group * WINDOW_REACH
    total_rows = group_rows * n_sp
    ctx_total = n_sp * ctx_rows
    contract = (((1,), (1,)), ((), ()))

    def attend(block):
        begin = pl.multiple_of(block * WINDOW_REACH, WINDOW_REACH)
        here = pl.ds(begin, WINDOW_REACH)
        around = pl.ds(begin, span)
        query_at = lax.rem(
            lax.broadcasted_iota(jnp.int32, (stacked, span), 0), WINDOW_REACH
        ) + WINDOW_REACH
        key_at = lax.broadcasted_iota(jnp.int32, (stacked, span), 1)
        key_pos = sp * group_rows + begin - WINDOW_REACH + key_at
        allowed = (
            (jnp.abs(key_at - query_at) <= WINDOW_REACH) & (key_pos >= 0) & (key_pos < total_rows)
        )
        for h in range(kv_local):
            heads = [h * per_group + i for i in range(per_group)]
            cols = slice(h * HEAD_DIM, (h + 1) * HEAD_DIM)
            value_cols = slice(pair + h * HEAD_DIM, pair + (h + 1) * HEAD_DIM)
            q = jnp.concatenate(
                [queries[here, i * HEAD_DIM : (i + 1) * HEAD_DIM] for i in heads], axis=0
            )
            band = lax.dot_general(q, kv[around, cols], contract, preferred_element_type=F32)
            band = jnp.where(allowed, band, MASKED_SCORE)
            ctx_keys = ctx_kv[:, :, cols].reshape(ctx_total, HEAD_DIM)
            ctx_values = ctx_kv[:, :, value_cols].reshape(ctx_total, HEAD_DIM)
            far = lax.dot_general(q, ctx_keys, contract, preferred_element_type=F32)
            sink = jnp.concatenate(
                [jnp.full((WINDOW_REACH, 1), sink_ref[0, i] * log2e, F32) for i in heads], axis=0
            )
            top = jnp.maximum(
                jnp.maximum(
                    jnp.max(band, axis=-1, keepdims=True), jnp.max(far, axis=-1, keepdims=True)
                ),
                sink,
            )
            band_exp = jnp.exp2(band - top)
            far_exp = jnp.exp2(far - top)
            total = (
                jnp.sum(band_exp, axis=-1, keepdims=True)
                + jnp.sum(far_exp, axis=-1, keepdims=True)
                + jnp.exp2(sink - top)
            )
            mixed = jnp.dot(
                band_exp.astype(BF16), kv[around, value_cols], preferred_element_type=F32
            ) + jnp.dot(far_exp.astype(BF16), ctx_values, preferred_element_type=F32)
            mixed = (mixed / total).astype(BF16)
            for n, i in enumerate(heads):
                attended[here, i * HEAD_DIM : (i + 1) * HEAD_DIM] = mixed[
                    n * WINDOW_REACH : (n + 1) * WINDOW_REACH
                ]

    by_part = rows % WINDOW_REACH == 0
    part_blocks = rows // WINDOW_REACH

    def attend_part(slot):
        if by_part:
            loop(0, part_blocks, lambda b: attend(slot * part_blocks + b))

    if not by_part:
        loop(0, group_rows // WINDOW_REACH, attend)
    loads[8].wait()
    out_tile = tile_of(width, 512)

    def out_copy(d, mine):
        peer = lax.rem(tp + d, n_tp)
        slot = tp if mine else peer
        return pltpu.make_async_remote_copy(
            src_ref=partial_out.at[peer],
            dst_ref=partial_in.at[slot],
            send_sem=out_send.at[peer],
            recv_sem=out_recv.at[slot],
            device_id={"tp": peer},
            device_id_type=MESH,
        )

    def project_out(slot, store):
        source = pl.ds(pl.multiple_of(slot * rows, strip), rows)

        def one(j):
            cols = pl.ds(pl.multiple_of(j * out_tile, out_tile), out_tile)
            store(
                cols,
                jnp.dot(attended[source, :], wo[:, cols], preferred_element_type=F32).astype(BF16),
            )

        loop(0, width // out_tile, one)

    def peer_part(d):
        slot = lax.rem(tp + d, n_tp)
        attend_part(slot)

        def store(cols, value):
            partial_out[slot, :, cols] = value

        project_out(slot, store)
        out_copy(d, True).start()

    loop(1, n_tp, peer_part)
    attend_part(tp)

    def keep(cols, value):
        own_total[:, cols] = value.astype(F32)

    project_out(tp, keep)
    loop(1, n_tp, lambda d: out_copy(d, False).wait_recv())

    def finish(i):
        at = pl.ds(pl.multiple_of(i * strip, strip), strip)
        mixed = own_total[at, :]
        for d in range(1, n_tp):
            mixed = mixed + partial_in[lax.rem(tp + d, n_tp), at, :].astype(F32)
        out_ref[at, :] = (latent[at, :].astype(F32) + mod[4:5, :] * mixed).astype(BF16)

    loop(0, rows // strip, finish)

    loop(1, n_sp, lambda d: rs_copy(d).wait_send())
    loop(1, everyone, lambda d: ag_copy(d).wait_send())
    loop(1, n_tp, lambda d: hid_copy(d, True).wait_send())
    loop(1, n_tp, lambda d: out_copy(d, True).wait_send())
    for copy in ctx_sends:
        copy.wait_send()

    if raw_halo:

        @pl.when(has_next & holds_last)
        def _():
            raw_copy(True, 0).wait_send()
            raw_copy(True, 1).wait_send()

        @pl.when(has_last & holds_first)
        def _():
            raw_copy(False, 0).wait_send()
            raw_copy(False, 1).wait_send()

        @pl.when(has_last & holds_last)
        def _():
            loop(1, n_tp, lambda d: edge_copy(True, d, True).wait_send())

        @pl.when(has_next & holds_first)
        def _():
            loop(1, n_tp, lambda d: edge_copy(False, d, True).wait_send())
    else:

        @pl.when(has_next)
        def _():
            halo_copy(True).wait_send()

        @pl.when(has_last)
        def _():
            halo_copy(False).wait_send()


def angle_tables(total_rows):
    inv_freq = np.power(
        10000.0, -np.arange(0, HEAD_DIM // 2, 2, dtype=np.float64) / (HEAD_DIM // 2)
    ).astype(np.float32)

    def tables(count):
        angle = (np.arange(count, dtype=np.float32)[:, None] * inv_freq).astype(np.float64)
        cosine, sine = np.cos(angle), np.sin(angle)
        return (
            np.concatenate([cosine, cosine], axis=1).astype(np.float32),
            np.concatenate([-sine, sine], axis=1).astype(np.float32),
        )

    empty = HEAD_DIM // 2
    by_row = [np.pad(t, ((0, 0), (0, empty))) for t in tables(total_rows // GRID_W)]
    by_col = [np.pad(t, ((0, 0), (empty, 0))) for t in tables(GRID_W)]
    return by_row + by_col


def shards(
    n_sp,
    n_tp,
    latent,
    condition,
    context_condition,
    context,
    norm_gain,
    shift_weight,
    scale_weight,
    gate_weight,
    query_weight,
    key_matrix,
    value_matrix,
    sink_logit_head,
    out_weight,
):
    rows, width = latent.shape
    group_rows = rows * n_tp
    angles = [jnp.asarray(t) for t in angle_tables(group_rows * n_sp)]
    columns = shift_weight.shape[1]
    groups = 5 * columns // LANES
    per = -(-groups // n_sp)
    query_width = query_weight.shape[1]
    pair = key_matrix.shape[1]
    ctx_rows = context.shape[0]
    lines = n_sp // QUAD
    ctx_sends = (lines - 1) + 4 * lines
    dma = pltpu.SemaphoreType.DMA
    vmem = pl.BlockSpec(memory_space=pltpu.VMEM)
    anywhere = pl.BlockSpec(memory_space=pl.ANY)

    def like(array):
        return pltpu.VMEM(array.shape, array.dtype)

    return pl.pallas_call(
        functools.partial(block_kernel, n_sp, n_tp),
        out_shape=jax.ShapeDtypeStruct((rows, width), BF16),
        in_specs=[vmem] * 7 + [pl.BlockSpec(memory_space=pltpu.SMEM)] + [anywhere] * 9,
        out_specs=vmem,
        scratch_shapes=[
            like(latent),
            like(context),
            like(shift_weight),
            like(scale_weight),
            like(gate_weight),
            like(query_weight),
            like(key_matrix),
            like(value_matrix),
            like(out_weight),
            pltpu.VMEM((n_sp, per, LANES), F32),
            pltpu.VMEM((n_sp, per, LANES), F32),
            pltpu.VMEM((n_tp, n_sp, per, LANES), F32),
            pltpu.VMEM((8, width), F32),
            pltpu.VMEM((group_rows + 2 * WINDOW_REACH, width), BF16),
            like(context),
            pltpu.VMEM((group_rows, query_width), BF16),
            pltpu.VMEM((group_rows + 2 * WINDOW_REACH, 2 * pair), BF16),
            pltpu.VMEM((n_sp, ctx_rows, 2 * pair), BF16),
            pltpu.VMEM((group_rows, query_width), BF16),
            pltpu.VMEM((n_tp, rows, width), BF16),
            pltpu.VMEM((n_tp, rows, width), BF16),
            pltpu.VMEM((rows, width), F32),
            pltpu.VMEM((group_rows + 2 * WINDOW_REACH, HEAD_DIM), F32),
            pltpu.VMEM((group_rows + 2 * WINDOW_REACH, HEAD_DIM), F32),
            pltpu.VMEM((2, WINDOW_REACH, width), BF16),
            dma((9,)),
            dma((n_sp,)),
            dma((n_sp,)),
            dma((n_tp, n_sp)),
            dma((n_tp, n_sp)),
            dma((n_tp,)),
            dma((n_tp,)),
            dma((ctx_sends,)),
            dma((n_sp, 2)),
            dma((2,)),
            dma((2,)),
            dma((2, 2)),
            dma((2, 2)),
            dma((2, n_tp)),
            dma((2,)),
            dma((n_tp,)),
            dma((n_tp,)),
        ],
        compiler_params=pltpu.CompilerParams(
            collective_id=0, has_side_effects=True, vmem_limit_bytes=63 * 1024 * 1024
        ),
    )(
        condition.reshape(1, -1),
        context_condition.reshape(1, -1),
        norm_gain.reshape(1, -1),
        *angles,
        sink_logit_head.reshape(1, -1),
        latent,
        context,
        shift_weight,
        scale_weight,
        gate_weight,
        query_weight,
        key_matrix,
        value_matrix,
        out_weight,
    )


def solution(mesh):
    placed = (
        P(("sp", "tp"), None),
        P("sp"),
        P("sp"),
        P("sp", None),
        P(),
        P("sp", "tp"),
        P("sp", "tp"),
        P("sp", "tp"),
        P(None, "tp"),
        P(None, "tp"),
        P(None, "tp"),
        P("tp"),
        P("tp", None),
    )
    return jax.shard_map(
        functools.partial(shards, mesh.shape["sp"], mesh.shape["tp"]),
        mesh=mesh,
        in_specs=placed,
        out_specs=P(("sp", "tp"), None),
        check_vma=False,
    )
```

```python
import functools

import jax
import jax.numpy as jnp
import numpy as np
from jax import lax
from jax.experimental import pallas as pl
from jax.experimental.pallas import tpu as pltpu
from jax.sharding import PartitionSpec as P

QUERY_HEADS = 16
KEY_VALUE_HEADS = 8
HEAD_DIM = 128
WINDOW_REACH = 128
GRID_W = 64
NORM_EPS = 1e-05
MASKED_SCORE = -1e30
LANES = 128
QUAD = 4
MESH = pl.DeviceIdType.MESH
F32 = jnp.float32
BF16 = jnp.bfloat16


def tile_of(extent, most):
    tile = min(extent, most)
    while extent % tile:
        tile -= LANES
    return tile


def block_kernel(
    n_sp,
    n_tp,
    cond_ref,
    ctx_cond_ref,
    gain_ref,
    row_cos,
    row_sin,
    col_cos,
    col_sin,
    sink_ref,
    latent_hbm,
    context_hbm,
    shift_hbm,
    scale_hbm,
    gate_hbm,
    wq_hbm,
    wk_hbm,
    wv_hbm,
    wo_hbm,
    out_ref,
    latent,
    context,
    shift_w,
    scale_w,
    gate_w,
    wq,
    wk,
    wv,
    wo,
    part,
    gathered,
    full,
    mod,
    hidden,
    ctx_hidden,
    queries,
    keys_kept,
    values_kept,
    values_t,
    ctx_kv,
    ctx_values_t,
    sums,
    tops,
    attended,
    partial_out,
    partial_in,
    own_total,
    cos_ref,
    sin_ref,
    load_sem,
    rs_send,
    rs_recv,
    ag_send,
    ag_recv,
    hid_send,
    hid_recv,
    ctx_send,
    ctx_recv,
    halo_send,
    halo_recv,
    out_send,
    out_recv,
):
    sp = lax.axis_index("sp")
    tp = lax.axis_index("tp")
    rows, width = latent.shape
    group_rows = rows * n_tp
    columns = shift_w.shape[1]
    chunks = columns // LANES
    per = part.shape[1]
    query_width = wq.shape[1]
    pair = wk.shape[1]
    kv_local = pair // HEAD_DIM
    per_group = query_width // pair
    ctx_rows = context.shape[0]

    loads = [
        pltpu.make_async_copy(src, dst, load_sem.at[i])
        for i, (src, dst) in enumerate(
            [
                (shift_hbm, shift_w),
                (scale_hbm, scale_w),
                (gate_hbm, gate_w),
                (context_hbm, context),
                (latent_hbm, latent),
                (wk_hbm, wk),
                (wv_hbm, wv),
                (wq_hbm, wq),
                (wo_hbm, wo),
            ]
        )
    ]
    for load in loads:
        load.start()

    barrier = pltpu.get_barrier_semaphore()

    everyone = n_sp * n_tp
    me = sp * n_tp + tp

    def other(d):
        at = lax.rem(me + d, everyone)
        return at // n_tp, lax.rem(at, n_tp)

    def greet(d, carry):
        peer_sp, peer_tp = other(d)
        pl.semaphore_signal(
            barrier, inc=1, device_id={"sp": peer_sp, "tp": peer_tp}, device_id_type=MESH
        )
        return carry

    lax.fori_loop(1, everyone, greet, 0)

    def silu(v):
        return v / (1.0 + jnp.exp(-v))

    depth = cond_ref.shape[1]
    row_id = lax.broadcasted_iota(jnp.int32, (16, depth), 0)
    active = jnp.where(
        row_id == 0,
        jnp.broadcast_to(silu(cond_ref[...]), (16, depth)),
        jnp.broadcast_to(silu(ctx_cond_ref[...]), (16, depth)),
    ).astype(BF16)
    part[...] = jnp.zeros_like(part)
    vector = 0
    for load, weight, count in zip(loads[:3], (shift_w, scale_w, gate_w), (2, 2, 1)):
        load.wait()
        product = jnp.dot(active, weight[...], preferred_element_type=F32)
        for v in range(count):
            for j in range(chunks):
                g = vector * chunks + j
                part[g // per, g % per : g % per + 1, :] = product[
                    v : v + 1, j * LANES : (j + 1) * LANES
                ]
            vector += 1

    pl.semaphore_wait(barrier, everyone - 1)

    def rs_copy(d):
        peer = lax.rem(sp + d, n_sp)
        return pltpu.make_async_remote_copy(
            src_ref=part.at[peer],
            dst_ref=gathered.at[sp],
            send_sem=rs_send.at[peer],
            recv_sem=rs_recv.at[sp],
            device_id={"sp": peer},
            device_id_type=MESH,
        )

    def rs_arrival(d):
        peer = lax.rem(sp + d, n_sp)
        return pltpu.make_async_remote_copy(
            src_ref=part.at[peer],
            dst_ref=gathered.at[peer],
            send_sem=rs_send.at[peer],
            recv_sem=rs_recv.at[peer],
            device_id={"sp": peer},
            device_id_type=MESH,
        )

    def loop(low, high, f):
        def step(i, carry):
            f(i)
            return carry

        lax.fori_loop(low, high, step, 0)

    has_next, has_last = sp < n_sp - 1, sp > 0

    loop(1, n_sp, lambda d: rs_copy(d).start())
    gathered[sp] = part[sp]
    loads[4].wait()

    strip = 32

    def scale_strip(i):
        at = pl.multiple_of(i * strip, strip)
        floats = latent[pl.ds(at, strip), :].astype(F32)
        inverse = lax.rsqrt(jnp.mean(floats * floats, axis=-1, keepdims=True) + NORM_EPS)
        own_total[pl.ds(at, strip), :] = floats * inverse

    loop(0, rows // strip, scale_strip)

    grid_rows = group_rows // GRID_W
    grid_pad = WINDOW_REACH // GRID_W
    in_row = lax.broadcasted_iota(jnp.int32, (GRID_W, HEAD_DIM), 1) < HEAD_DIM // 2

    def fill_angles(i):
        row = jnp.clip(sp * grid_rows - grid_pad + i, 0, n_sp * grid_rows - 1)
        at = pl.ds(pl.multiple_of(i * GRID_W, GRID_W), GRID_W)
        for target, by_row, by_col in ((cos_ref, row_cos, col_cos), (sin_ref, row_sin, col_sin)):
            spread = jnp.broadcast_to(by_row[pl.ds(row, 1), :], (GRID_W, HEAD_DIM))
            target[at, :] = jnp.where(in_row, spread, by_col[...])

    loop(0, grid_rows + 2 * grid_pad, fill_angles)
    loop(1, n_sp, lambda d: rs_arrival(d).wait_recv())
    full[tp, sp] = jnp.sum(gathered[...], axis=0)

    def ag_copy(d):
        peer_sp, peer_tp = other(d)
        return pltpu.make_async_remote_copy(
            src_ref=full.at[tp, sp],
            dst_ref=full.at[tp, sp],
            send_sem=ag_send.at[peer_tp, peer_sp],
            recv_sem=ag_recv.at[tp, sp],
            device_id={"sp": peer_sp, "tp": peer_tp},
            device_id_type=MESH,
        )

    def ag_arrival(d):
        peer_sp, peer_tp = other(d)
        return pltpu.make_async_remote_copy(
            src_ref=full.at[tp, sp],
            dst_ref=full.at[peer_tp, peer_sp],
            send_sem=ag_send.at[peer_tp, peer_sp],
            recv_sem=ag_recv.at[peer_tp, peer_sp],
            device_id={"sp": peer_sp, "tp": peer_tp},
            device_id_type=MESH,
        )

    loop(1, everyone, lambda d: ag_copy(d).start())

    loop(1, everyone, lambda d: ag_arrival(d).wait_recv())

    for t in range(n_tp):
        for v in range(5):
            for j in range(chunks):
                g = v * chunks + j
                column = t * columns + j * LANES
                mod[v : v + 1, column : column + LANES] = full[t, g // per, g % per : g % per + 1, :]
    gain = gain_ref[...]
    mod[2:3, :] = gain * (1.0 + mod[2:3, :])
    mod[3:4, :] = gain * (1.0 + mod[3:4, :])

    def normed(block, shift_row, scale_row):
        floats = block.astype(F32)
        inverse = lax.rsqrt(jnp.mean(floats * floats, axis=-1, keepdims=True) + NORM_EPS)
        return (
            floats * inverse * mod[scale_row : scale_row + 1, :] + mod[shift_row : shift_row + 1, :]
        ).astype(BF16)

    for i in (3, 5, 6):
        loads[i].wait()
    ctx_hidden[...] = normed(context[...], 1, 3)
    tile = tile_of(pair, 512)

    def ctx_project(j):
        at = pl.multiple_of(j * tile, tile)
        ctx_kv[sp, :, pl.ds(at, tile)] = jnp.dot(
            ctx_hidden[...], wk[:, pl.ds(at, tile)], preferred_element_type=F32
        ).astype(BF16)
        ctx_kv[sp, :, pl.ds(pl.multiple_of(pair + at, tile), tile)] = jnp.dot(
            ctx_hidden[...], wv[:, pl.ds(at, tile)], preferred_element_type=F32
        ).astype(BF16)

    loop(0, pair // tile, ctx_project)

    lines = n_sp // QUAD
    line, corner = sp // QUAD, lax.rem(sp, QUAD)

    across = corner + 1 - 2 * lax.rem(corner, 2)
    beside = lax.rem(corner + 2, QUAD)
    opposite = QUAD - 1 - corner

    def ctx_copy(slot, peer, sem, half=None):
        cols = slice(None) if half is None else pl.ds(half * pair, pair)
        return pltpu.make_async_remote_copy(
            src_ref=ctx_kv.at[slot, :, cols],
            dst_ref=ctx_kv.at[slot, :, cols],
            send_sem=ctx_send.at[sem],
            recv_sem=ctx_recv.at[slot, half or 0],
            device_id={"sp": peer},
            device_id_type=MESH,
        )

    ctx_sends = []

    def send_ctx(slot, peer, half=None):
        copy = ctx_copy(slot, peer, len(ctx_sends), half)
        copy.start()
        ctx_sends.append(copy)

    def send_quad(slot):
        send_ctx(slot, line * QUAD + across)
        send_ctx(slot, line * QUAD + beside)

    for d in range(1, lines):
        send_ctx(sp, lax.rem(line + d, lines) * QUAD + corner)
    send_quad(sp)

    def line_base(d):
        return lax.rem(line + lines - d, lines) * QUAD

    def forward(d):
        slot = line_base(d) + corner
        ctx_copy(slot, sp, 0).wait_recv()
        send_quad(slot)

    def relay(d):
        ctx_copy(line_base(d) + across, sp, 0).wait_recv()
        send_ctx(line_base(d) + across, line * QUAD + beside, 0)
        ctx_copy(line_base(d) + beside, sp, 0).wait_recv()
        send_ctx(line_base(d) + beside, line * QUAD + across, 1)

    def serve(step):
        if step < lines:
            if step + 1 < lines:
                forward(step + 1)
            relay(step)

    own_start = pl.multiple_of(WINDOW_REACH + tp * rows, strip)

    def norm_strip(i):
        at = pl.multiple_of(i * strip, strip)
        hidden[pl.ds(pl.multiple_of(own_start + at, strip), strip), :] = (
            own_total[pl.ds(at, strip), :] * mod[2:3, :] + mod[0:1, :]
        ).astype(BF16)

    loop(0, rows // strip, norm_strip)

    def hid_copy(d, mine):
        peer = lax.rem(tp + d, n_tp)
        slot = tp if mine else peer
        at = pl.multiple_of(WINDOW_REACH + slot * rows, strip)
        mine_at = pl.multiple_of(WINDOW_REACH + tp * rows, strip)
        return pltpu.make_async_remote_copy(
            src_ref=hidden.at[pl.ds(mine_at, rows)],
            dst_ref=hidden.at[pl.ds(at, rows)],
            send_sem=hid_send.at[peer],
            recv_sem=hid_recv.at[slot],
            device_id={"tp": peer},
            device_id_type=MESH,
        )

    loop(1, n_tp, lambda d: hid_copy(d, True).start())

    quarter = HEAD_DIM // 4
    def turned(values, cosine, sine):
        pieces = []
        lane = lax.broadcasted_iota(jnp.int32, cosine.shape, 1)
        low_half = lax.rem(lane, 2 * quarter) < quarter
        for h in range(values.shape[1] // HEAD_DIM):
            u = values[:, h * HEAD_DIM : (h + 1) * HEAD_DIM]
            other = jnp.where(
                low_half, pltpu.roll(u, HEAD_DIM - quarter, 1), pltpu.roll(u, quarter, 1)
            )
            pieces.append(u * cosine + other * sine)
        return jnp.concatenate(pieces, axis=1).astype(BF16)

    aligned = rows % WINDOW_REACH == 0

    def project_kv(start):
        source = pl.ds(pl.multiple_of(start, strip), rows)

        def one(j):
            col = pl.multiple_of(j * tile, tile)
            keys = jnp.dot(hidden[source, :], wk[:, pl.ds(col, tile)], preferred_element_type=F32)
            keys_kept[source, pl.ds(col, tile)] = turned(keys, cos_ref[source, :], sin_ref[source, :])
            values = jnp.dot(hidden[source, :], wv[:, pl.ds(col, tile)], preferred_element_type=F32)
            if aligned:
                at = pl.ds(pl.multiple_of(start, WINDOW_REACH), rows)
                values_t[pl.ds(col, tile), at] = values.astype(BF16).T
            else:
                values_kept[source, pl.ds(col, tile)] = values.astype(BF16)

        loop(0, pair // tile, one)

    def transpose_values():
        if not aligned:

            def one(i):
                at = pl.ds(pl.multiple_of(WINDOW_REACH * (i + 1), WINDOW_REACH), WINDOW_REACH)
                values_t[:, at] = values_kept[at, :].T

            loop(0, group_rows // WINDOW_REACH, one)

    def project_q(slot):
        target = pl.ds(pl.multiple_of(slot * rows, strip), rows)
        source = pl.ds(pl.multiple_of(WINDOW_REACH + slot * rows, strip), rows)
        q_tile = tile_of(query_width, 512)

        def one(j):
            col = pl.multiple_of(j * q_tile, q_tile)
            q = jnp.dot(hidden[source, :], wq[:, pl.ds(col, q_tile)], preferred_element_type=F32)
            queries[target, pl.ds(col, q_tile)] = turned(
                q * factor, cos_ref[source, :], sin_ref[source, :]
            )

        loop(0, query_width // q_tile, one)

    log2e = 1.4426950408889634
    factor = HEAD_DIM ** (-0.5) * log2e
    def halo_copies(up):
        source = group_rows if up else WINDOW_REACH
        target = 0 if up else group_rows + WINDOW_REACH
        which = 0 if up else 1
        peer = {"sp": lax.rem(sp + (1 if up else n_sp - 1), n_sp)}
        ends = (
            (keys_kept.at[pl.ds(source, WINDOW_REACH)], keys_kept.at[pl.ds(target, WINDOW_REACH)]),
            (
                values_t.at[:, pl.ds(source, WINDOW_REACH)],
                values_t.at[:, pl.ds(target, WINDOW_REACH)],
            ),
        )
        return [
            pltpu.make_async_remote_copy(
                src_ref=src,
                dst_ref=dst,
                send_sem=halo_send.at[which, i],
                recv_sem=halo_recv.at[which, i],
                device_id=peer,
                device_id_type=MESH,
            )
            for i, (src, dst) in enumerate(ends)
        ]

    def send_halo():
        @pl.when(has_next)
        def _():
            for copy in halo_copies(True):
                copy.start()

        @pl.when(has_last)
        def _():
            for copy in halo_copies(False):
                copy.start()

        def clear(at):
            region = pl.ds(at, WINDOW_REACH)
            keys_kept[region, :] = jnp.zeros((WINDOW_REACH, pair), BF16)
            values_t[:, region] = jnp.zeros((pair, WINDOW_REACH), BF16)

        @pl.when(jnp.logical_not(has_last))
        def _():
            clear(0)

        @pl.when(jnp.logical_not(has_next))
        def _():
            clear(group_rows + WINDOW_REACH)

    def receive_halo():
        @pl.when(has_last)
        def _():
            for copy in halo_copies(True):
                copy.wait_recv()

        @pl.when(has_next)
        def _():
            for copy in halo_copies(False):
                copy.wait_recv()

    span = 3 * WINDOW_REACH
    stacked = per_group * WINDOW_REACH
    contract = (((1,), (1,)), ((), ()))
    blocks = group_rows // WINDOW_REACH
    lines_each = max(1, 256 // (QUAD * ctx_rows))
    ctx_chunks = lines // lines_each
    slots_each = QUAD * lines_each
    chunk_rows = slots_each * ctx_rows
    ahead = lax.rem(
        lax.broadcasted_iota(jnp.int32, (WINDOW_REACH, stacked), 1), WINDOW_REACH
    ) - lax.broadcasted_iota(jnp.int32, (WINDOW_REACH, stacked), 0)
    WINDOW = "window"

    def chunk_at(k):
        return lax.rem(line // lines_each + ctx_chunks - k, ctx_chunks)

    def query_heads(h):
        return range(h * per_group, (h + 1) * per_group)

    def scores(block, h, piece):
        begin = pl.multiple_of(block * WINDOW_REACH, WINDOW_REACH)
        cols = slice(h * HEAD_DIM, (h + 1) * HEAD_DIM)
        q = jnp.concatenate(
            [
                queries[pl.ds(begin, WINDOW_REACH), i * HEAD_DIM : (i + 1) * HEAD_DIM]
                for i in query_heads(h)
            ],
            axis=0,
        )
        if piece is not WINDOW:
            keys = ctx_kv[pl.ds(piece * slots_each, slots_each), :, cols]
            keys = keys.reshape(chunk_rows, HEAD_DIM)
            return lax.dot_general(keys, q, contract, preferred_element_type=F32)
        keys = keys_kept[pl.ds(begin, span), cols]
        band = lax.dot_general(keys, q, contract, preferred_element_type=F32)
        lowest = jnp.where((block > 0) | has_last, 0, -span)
        highest = jnp.where((block < blocks - 1) | has_next, 0, span)
        return jnp.concatenate(
            [
                jnp.where(ahead <= lowest, band[:WINDOW_REACH], MASKED_SCORE),
                band[WINDOW_REACH : 2 * WINDOW_REACH],
                jnp.where(ahead >= highest, band[2 * WINDOW_REACH :], MASKED_SCORE),
            ],
            axis=0,
        )

    def weighted(block, h, piece, probs):
        cols = slice(h * HEAD_DIM, (h + 1) * HEAD_DIM)
        if piece is WINDOW:
            begin = pl.multiple_of(block * WINDOW_REACH, WINDOW_REACH)
            values = values_t[cols, pl.ds(begin, span)]
        else:
            begin = pl.multiple_of(piece * chunk_rows, chunk_rows)
            values = ctx_values_t[cols, pl.ds(begin, chunk_rows)]
        ones = jnp.ones((16, probs.shape[0]), BF16)
        return jnp.dot(
            jnp.concatenate([values, ones], axis=0), probs, preferred_element_type=F32
        )[: HEAD_DIM + 8]

    def sinks(h):
        return jnp.concatenate(
            [jnp.full((1, WINDOW_REACH), sink_ref[0, i] * log2e, F32) for i in query_heads(h)],
            axis=1,
        )

    def attend(items, first=False, last=False):
        tasks = [(b, h, pieces) for b, pieces in items for h in range(kv_local)]
        top, total = {}, {}
        following = {i: scores(b, h, pieces[0]) for i, (b, h, pieces) in enumerate(tasks)}
        for step in range(max(len(pieces) for _, pieces in items)):
            current, following, now = following, {}, {}
            live = [(i, *task) for i, task in enumerate(tasks) if step < len(task[2])]
            for i, b, h, pieces in live:
                if step + 1 < len(pieces):
                    following[i] = scores(b, h, pieces[step + 1])
            for i, b, h, pieces in live:
                if step == 0:
                    top[i] = sinks(h) if first else tops[b, h, 0:1, :]
                now[i] = jnp.maximum(top[i], jnp.max(current[i], axis=0, keepdims=True))
            probs = {i: jnp.exp2(current[i] - now[i]).astype(BF16) for i, *_ in live}
            for i, b, h, pieces in live:
                added = weighted(b, h, pieces[step], probs[i])
                shrink = jnp.exp2(top[i] - now[i])
                if step == 0 and first:
                    total[i] = jnp.concatenate(
                        [added[:HEAD_DIM], added[HEAD_DIM:] + shrink], axis=0
                    )
                else:
                    total[i] = (sums[b, h] if step == 0 else total[i]) * shrink + added
                top[i] = now[i]
        for i, (b, h, pieces) in enumerate(tasks):
            if last:
                mixed = total[i][:HEAD_DIM] / total[i][HEAD_DIM : HEAD_DIM + 1]
                mixed = mixed.T.astype(BF16)
                here = pl.ds(pl.multiple_of(b * WINDOW_REACH, WINDOW_REACH), WINDOW_REACH)
                for n, k in enumerate(query_heads(h)):
                    attended[here, k * HEAD_DIM : (k + 1) * HEAD_DIM] = mixed[
                        n * WINDOW_REACH : (n + 1) * WINDOW_REACH
                    ]
            else:
                sums[b, h] = total[i]
                tops[b, h, 0:1, :] = top[i]

    def attend_all(n, first_block, pieces, most, **kind):
        each = max(i for i in range(1, most + 1) if n % i == 0)
        loop(
            0,
            n // each,
            lambda g: attend([(first_block + g * each + i, pieces) for i in range(each)], **kind),
        )

    def start_block(b):
        for h in range(kv_local):
            sums[b, h, :HEAD_DIM, :] = jnp.zeros((HEAD_DIM, stacked), F32)
            sums[b, h, HEAD_DIM:, :] = jnp.ones((8, stacked), F32)
            tops[b, h, 0:1, :] = sinks(h)

    def opposite_arrived(base):
        for half in range(2):
            ctx_copy(base + opposite, sp, 0, half).wait_recv()

    def transpose_chunk(piece):
        values = ctx_kv[pl.ds(piece * slots_each, slots_each), :, pl.ds(pair, pair)]
        at = pl.multiple_of(piece * chunk_rows, chunk_rows)
        ctx_values_t[:, pl.ds(at, chunk_rows)] = values.reshape(chunk_rows, pair).T

    def receive_chunk(k):
        if lines_each == 1:
            opposite_arrived(line_base(k))
        elif k == 0:
            loop(0, lines, lambda i: opposite_arrived(i * QUAD))
        transpose_chunk(chunk_at(k))

    early = aligned and n_tp == 2 and blocks >= 6
    inner = blocks - 2

    project_kv(WINDOW_REACH + tp * rows)
    loop(1, n_tp, lambda d: hid_copy(d, False).wait_recv())
    loop(1, n_tp, lambda d: project_kv(WINDOW_REACH + lax.rem(tp + d, n_tp) * rows))
    transpose_values()
    serve(0)
    loads[7].wait()
    project_q(tp)
    serve(1)
    loop(1, n_tp, lambda d: project_q(lax.rem(tp + d, n_tp)))
    if early:
        attend_all(inner, 1, [WINDOW], 2, first=True)
        start_block(0)
        start_block(blocks - 1)
    else:
        loop(0, blocks, start_block)
    serve(2)
    send_halo()
    if lines_each > 1:
        for step in range(3, lines):
            serve(step)
    receive_chunk(0)
    attend_all(blocks, 0, [chunk_at(0)], 3)
    if lines_each == 1:
        for step in range(3, lines):
            serve(step)
    for k in range(1, ctx_chunks - 1):
        receive_chunk(k)
        attend_all(blocks, 0, [chunk_at(k)], 3)
    receive_chunk(ctx_chunks - 1)
    receive_halo()
    final = chunk_at(ctx_chunks - 1)

    part_blocks = rows // WINDOW_REACH

    def finish_part(slot):
        if early:
            edge = slot * (blocks - 1)
            from_block = slot * part_blocks + 1 - slot
            inside = [(from_block + i, [final]) for i in range(part_blocks - 1)]
            attend(inside + [(edge, [final, WINDOW])], last=True)

    if not early:
        attend_all(blocks, 0, [final, WINDOW], 2, last=True)
    loads[8].wait()
    out_tile = tile_of(width, 512)

    def out_copy(d, mine):
        peer = lax.rem(tp + d, n_tp)
        slot = tp if mine else peer
        return pltpu.make_async_remote_copy(
            src_ref=partial_out.at[peer],
            dst_ref=partial_in.at[slot],
            send_sem=out_send.at[peer],
            recv_sem=out_recv.at[slot],
            device_id={"tp": peer},
            device_id_type=MESH,
        )

    def project_out(slot, store):
        source = pl.ds(pl.multiple_of(slot * rows, strip), rows)

        def one(j):
            cols = pl.ds(pl.multiple_of(j * out_tile, out_tile), out_tile)
            store(
                cols,
                jnp.dot(attended[source, :], wo[:, cols], preferred_element_type=F32).astype(BF16),
            )

        loop(0, width // out_tile, one)

    def peer_part(d):
        slot = lax.rem(tp + d, n_tp)
        finish_part(slot)

        def store(cols, value):
            partial_out[slot, :, cols] = value

        project_out(slot, store)
        out_copy(d, True).start()

    loop(1, n_tp, peer_part)
    finish_part(tp)

    def keep(cols, value):
        own_total[:, cols] = value.astype(F32)

    project_out(tp, keep)
    loop(1, n_tp, lambda d: out_copy(d, False).wait_recv())

    def finish(i):
        at = pl.ds(pl.multiple_of(i * strip, strip), strip)
        mixed = own_total[at, :]
        for d in range(1, n_tp):
            mixed = mixed + partial_in[lax.rem(tp + d, n_tp), at, :].astype(F32)
        out_ref[at, :] = (latent[at, :].astype(F32) + mod[4:5, :] * mixed).astype(BF16)

    loop(0, rows // strip, finish)

    loop(1, n_sp, lambda d: rs_copy(d).wait_send())
    loop(1, everyone, lambda d: ag_copy(d).wait_send())
    loop(1, n_tp, lambda d: hid_copy(d, True).wait_send())
    loop(1, n_tp, lambda d: out_copy(d, True).wait_send())
    for copy in ctx_sends:
        copy.wait_send()

    @pl.when(has_next)
    def _():
        for copy in halo_copies(True):
            copy.wait_send()

    @pl.when(has_last)
    def _():
        for copy in halo_copies(False):
            copy.wait_send()


def angle_tables(total_rows):
    inv_freq = np.power(
        10000.0, -np.arange(0, HEAD_DIM // 2, 2, dtype=np.float64) / (HEAD_DIM // 2)
    ).astype(np.float32)

    def tables(count):
        angle = (np.arange(count, dtype=np.float32)[:, None] * inv_freq).astype(np.float64)
        cosine, sine = np.cos(angle), np.sin(angle)
        return (
            np.concatenate([cosine, cosine], axis=1).astype(np.float32),
            np.concatenate([-sine, sine], axis=1).astype(np.float32),
        )

    empty = HEAD_DIM // 2
    by_row = [np.pad(t, ((0, 0), (0, empty))) for t in tables(total_rows // GRID_W)]
    by_col = [np.pad(t, ((0, 0), (empty, 0))) for t in tables(GRID_W)]
    return by_row + by_col


def shards(
    n_sp,
    n_tp,
    latent,
    condition,
    context_condition,
    context,
    norm_gain,
    shift_weight,
    scale_weight,
    gate_weight,
    query_weight,
    key_matrix,
    value_matrix,
    sink_logit_head,
    out_weight,
):
    rows, width = latent.shape
    group_rows = rows * n_tp
    angles = [jnp.asarray(t) for t in angle_tables(group_rows * n_sp)]
    columns = shift_weight.shape[1]
    groups = 5 * columns // LANES
    per = -(-groups // n_sp)
    query_width = query_weight.shape[1]
    pair = key_matrix.shape[1]
    ctx_rows = context.shape[0]
    lines = n_sp // QUAD
    ctx_sends = (lines - 1) + 4 * lines
    padded = group_rows + 2 * WINDOW_REACH
    state = (group_rows // WINDOW_REACH, pair // HEAD_DIM)
    stacked = query_width // pair * WINDOW_REACH
    dma = pltpu.SemaphoreType.DMA
    vmem = pl.BlockSpec(memory_space=pltpu.VMEM)
    anywhere = pl.BlockSpec(memory_space=pl.ANY)

    def like(array):
        return pltpu.VMEM(array.shape, array.dtype)

    return pl.pallas_call(
        functools.partial(block_kernel, n_sp, n_tp),
        out_shape=jax.ShapeDtypeStruct((rows, width), BF16),
        in_specs=[vmem] * 7 + [pl.BlockSpec(memory_space=pltpu.SMEM)] + [anywhere] * 9,
        out_specs=vmem,
        scratch_shapes=[
            like(latent),
            like(context),
            like(shift_weight),
            like(scale_weight),
            like(gate_weight),
            like(query_weight),
            like(key_matrix),
            like(value_matrix),
            like(out_weight),
            pltpu.VMEM((n_sp, per, LANES), F32),
            pltpu.VMEM((n_sp, per, LANES), F32),
            pltpu.VMEM((n_tp, n_sp, per, LANES), F32),
            pltpu.VMEM((8, width), F32),
            pltpu.VMEM((group_rows + 2 * WINDOW_REACH, width), BF16),
            like(context),
            pltpu.VMEM((group_rows, query_width), BF16),
            pltpu.VMEM((padded, pair), BF16),
            pltpu.VMEM((8 if rows % WINDOW_REACH == 0 else padded, pair), BF16),
            pltpu.VMEM((pair, padded), BF16),
            pltpu.VMEM((n_sp, ctx_rows, 2 * pair), BF16),
            pltpu.VMEM((pair, n_sp * ctx_rows), BF16),
            pltpu.VMEM((*state, HEAD_DIM + 8, stacked), F32),
            pltpu.VMEM((*state, 8, stacked), F32),
            pltpu.VMEM((group_rows, query_width), BF16),
            pltpu.VMEM((n_tp, rows, width), BF16),
            pltpu.VMEM((n_tp, rows, width), BF16),
            pltpu.VMEM((rows, width), F32),
            pltpu.VMEM((group_rows + 2 * WINDOW_REACH, HEAD_DIM), F32),
            pltpu.VMEM((group_rows + 2 * WINDOW_REACH, HEAD_DIM), F32),
            dma((9,)),
            dma((n_sp,)),
            dma((n_sp,)),
            dma((n_tp, n_sp)),
            dma((n_tp, n_sp)),
            dma((n_tp,)),
            dma((n_tp,)),
            dma((ctx_sends,)),
            dma((n_sp, 2)),
            dma((2, 2)),
            dma((2, 2)),
            dma((n_tp,)),
            dma((n_tp,)),
        ],
        compiler_params=pltpu.CompilerParams(
            collective_id=0, has_side_effects=True, vmem_limit_bytes=63 * 1024 * 1024
        ),
    )(
        condition.reshape(1, -1),
        context_condition.reshape(1, -1),
        norm_gain.reshape(1, -1),
        *angles,
        sink_logit_head.reshape(1, -1),
        latent,
        context,
        shift_weight,
        scale_weight,
        gate_weight,
        query_weight,
        key_matrix,
        value_matrix,
        out_weight,
    )


def solution(mesh):
    placed = (
        P(("sp", "tp"), None),
        P("sp"),
        P("sp"),
        P("sp", None),
        P(),
        P("sp", "tp"),
        P("sp", "tp"),
        P("sp", "tp"),
        P(None, "tp"),
        P(None, "tp"),
        P(None, "tp"),
        P("tp"),
        P("tp", None),
    )
    return jax.shard_map(
        functools.partial(shards, mesh.shape["sp"], mesh.shape["tp"]),
        mesh=mesh,
        in_specs=placed,
        out_specs=P(("sp", "tp"), None),
        check_vma=False,
    )
```

```python
import functools

import jax
import jax.numpy as jnp
import numpy as np
from jax import lax
from jax.experimental import pallas as pl
from jax.experimental.pallas import tpu as pltpu
from jax.sharding import PartitionSpec as P

QUERY_HEADS = 16
KEY_VALUE_HEADS = 8
HEAD_DIM = 128
WINDOW_REACH = 128
GRID_W = 64
NORM_EPS = 1e-05
MASKED_SCORE = -1e30
LANES = 128
QUAD = 4
MESH = pl.DeviceIdType.MESH
F32 = jnp.float32
BF16 = jnp.bfloat16


def tile_of(extent, most):
    tile = min(extent, most)
    while extent % tile:
        tile -= LANES
    return tile


def block_kernel(
    n_sp,
    n_tp,
    cond_ref,
    ctx_cond_ref,
    gain_ref,
    row_cos,
    row_sin,
    col_cos,
    col_sin,
    sink_ref,
    latent_hbm,
    context_hbm,
    shift_hbm,
    scale_hbm,
    gate_hbm,
    wq_hbm,
    wk_hbm,
    wv_hbm,
    wo_hbm,
    out_ref,
    latent,
    context,
    shift_w,
    scale_w,
    gate_w,
    wq,
    wk,
    wv,
    wo,
    part,
    gathered,
    full,
    mod,
    hidden,
    ctx_hidden,
    queries,
    keys_kept,
    values_kept,
    values_t,
    ctx_kv,
    ctx_values_t,
    sums,
    tops,
    attended,
    partial_out,
    partial_in,
    own_total,
    cos_ref,
    sin_ref,
    halo_raw,
    edge_hidden,
    load_sem,
    rs_send,
    rs_recv,
    ag_send,
    ag_recv,
    hid_send,
    hid_recv,
    ctx_send,
    ctx_recv,
    halo_send,
    halo_recv,
    edge_send,
    edge_recv,
    out_send,
    out_recv,
):
    sp = lax.axis_index("sp")
    tp = lax.axis_index("tp")
    rows, width = latent.shape
    group_rows = rows * n_tp
    columns = shift_w.shape[1]
    chunks = columns // LANES
    per = part.shape[1]
    query_width = wq.shape[1]
    pair = wk.shape[1]
    kv_local = pair // HEAD_DIM
    per_group = query_width // pair
    ctx_rows = context.shape[0]

    loads = [
        pltpu.make_async_copy(src, dst, load_sem.at[i])
        for i, (src, dst) in enumerate(
            [
                (shift_hbm, shift_w),
                (scale_hbm, scale_w),
                (gate_hbm, gate_w),
                (context_hbm, context),
                (latent_hbm, latent),
                (wk_hbm, wk),
                (wv_hbm, wv),
                (wq_hbm, wq),
                (wo_hbm, wo),
            ]
        )
    ]
    for load in loads:
        load.start()

    barrier = pltpu.get_barrier_semaphore()

    everyone = n_sp * n_tp
    me = sp * n_tp + tp

    def other(d):
        at = lax.rem(me + d, everyone)
        return at // n_tp, lax.rem(at, n_tp)

    def greet(d, carry):
        peer_sp, peer_tp = other(d)
        pl.semaphore_signal(
            barrier, inc=1, device_id={"sp": peer_sp, "tp": peer_tp}, device_id_type=MESH
        )
        return carry

    lax.fori_loop(1, everyone, greet, 0)

    def silu(v):
        return v / (1.0 + jnp.exp(-v))

    depth = cond_ref.shape[1]
    row_id = lax.broadcasted_iota(jnp.int32, (16, depth), 0)
    active = jnp.where(
        row_id == 0,
        jnp.broadcast_to(silu(cond_ref[...]), (16, depth)),
        jnp.broadcast_to(silu(ctx_cond_ref[...]), (16, depth)),
    ).astype(BF16)
    part[...] = jnp.zeros_like(part)
    vector = 0
    for load, weight, count in zip(loads[:3], (shift_w, scale_w, gate_w), (2, 2, 1)):
        load.wait()
        product = jnp.dot(active, weight[...], preferred_element_type=F32)
        for v in range(count):
            for j in range(chunks):
                g = vector * chunks + j
                part[g // per, g % per : g % per + 1, :] = product[
                    v : v + 1, j * LANES : (j + 1) * LANES
                ]
            vector += 1

    pl.semaphore_wait(barrier, everyone - 1)

    def rs_copy(d):
        peer = lax.rem(sp + d, n_sp)
        return pltpu.make_async_remote_copy(
            src_ref=part.at[peer],
            dst_ref=gathered.at[sp],
            send_sem=rs_send.at[peer],
            recv_sem=rs_recv.at[sp],
            device_id={"sp": peer},
            device_id_type=MESH,
        )

    def rs_arrival(d):
        peer = lax.rem(sp + d, n_sp)
        return pltpu.make_async_remote_copy(
            src_ref=part.at[peer],
            dst_ref=gathered.at[peer],
            send_sem=rs_send.at[peer],
            recv_sem=rs_recv.at[peer],
            device_id={"sp": peer},
            device_id_type=MESH,
        )

    def loop(low, high, f):
        def step(i, carry):
            f(i)
            return carry

        lax.fori_loop(low, high, step, 0)

    has_next, has_last = sp < n_sp - 1, sp > 0
    holds_last, holds_first = tp == n_tp - 1, tp == 0
    raw_halo = rows >= WINDOW_REACH
    half_reach = WINDOW_REACH // 2

    def raw_copy(up, half):
        which = 0 if up else 1
        base = rows - WINDOW_REACH if up else 0
        return pltpu.make_async_remote_copy(
            src_ref=latent.at[pl.ds(base + half * half_reach, half_reach)],
            dst_ref=halo_raw.at[which, pl.ds(half * half_reach, half_reach)],
            send_sem=halo_send.at[which, half],
            recv_sem=halo_recv.at[which, half],
            device_id={"sp": lax.rem(sp + (1 if up else n_sp - 1), n_sp)},
            device_id_type=MESH,
        )

    def send_raw(half):
        if raw_halo:

            @pl.when(has_next & holds_last)
            def _():
                raw_copy(True, half).start()

            @pl.when(has_last & holds_first)
            def _():
                raw_copy(False, half).start()

    loop(1, n_sp, lambda d: rs_copy(d).start())
    gathered[sp] = part[sp]
    loads[4].wait()
    loop(1, n_sp, lambda d: rs_copy(d).wait_send())
    send_raw(0)

    strip = 32

    def scale_strip(i):
        at = pl.multiple_of(i * strip, strip)
        floats = latent[pl.ds(at, strip), :].astype(F32)
        inverse = lax.rsqrt(jnp.mean(floats * floats, axis=-1, keepdims=True) + NORM_EPS)
        own_total[pl.ds(at, strip), :] = floats * inverse

    loop(0, rows // strip, scale_strip)

    grid_rows = group_rows // GRID_W
    grid_pad = WINDOW_REACH // GRID_W
    in_row = lax.broadcasted_iota(jnp.int32, (GRID_W, HEAD_DIM), 1) < HEAD_DIM // 2

    def fill_angles(i):
        row = jnp.clip(sp * grid_rows - grid_pad + i, 0, n_sp * grid_rows - 1)
        at = pl.ds(pl.multiple_of(i * GRID_W, GRID_W), GRID_W)
        for target, by_row, by_col in ((cos_ref, row_cos, col_cos), (sin_ref, row_sin, col_sin)):
            spread = jnp.broadcast_to(by_row[pl.ds(row, 1), :], (GRID_W, HEAD_DIM))
            target[at, :] = jnp.where(in_row, spread, by_col[...])

    loop(0, grid_rows + 2 * grid_pad, fill_angles)
    loop(1, n_sp, lambda d: rs_arrival(d).wait_recv())
    full[tp, sp] = jnp.sum(gathered[...], axis=0)

    def ag_copy(d):
        peer_sp, peer_tp = other(d)
        return pltpu.make_async_remote_copy(
            src_ref=full.at[tp, sp],
            dst_ref=full.at[tp, sp],
            send_sem=ag_send.at[peer_tp, peer_sp],
            recv_sem=ag_recv.at[tp, sp],
            device_id={"sp": peer_sp, "tp": peer_tp},
            device_id_type=MESH,
        )

    def ag_arrival(d):
        peer_sp, peer_tp = other(d)
        return pltpu.make_async_remote_copy(
            src_ref=full.at[tp, sp],
            dst_ref=full.at[peer_tp, peer_sp],
            send_sem=ag_send.at[peer_tp, peer_sp],
            recv_sem=ag_recv.at[peer_tp, peer_sp],
            device_id={"sp": peer_sp, "tp": peer_tp},
            device_id_type=MESH,
        )

    loop(1, everyone, lambda d: ag_copy(d).start())
    loop(1, everyone, lambda d: ag_copy(d).wait_send())
    send_raw(1)

    loop(1, everyone, lambda d: ag_arrival(d).wait_recv())

    for t in range(n_tp):
        for v in range(5):
            for j in range(chunks):
                g = v * chunks + j
                column = t * columns + j * LANES
                mod[v : v + 1, column : column + LANES] = full[t, g // per, g % per : g % per + 1, :]
    gain = gain_ref[...]
    mod[2:3, :] = gain * (1.0 + mod[2:3, :])
    mod[3:4, :] = gain * (1.0 + mod[3:4, :])

    def normed(block, shift_row, scale_row):
        floats = block.astype(F32)
        inverse = lax.rsqrt(jnp.mean(floats * floats, axis=-1, keepdims=True) + NORM_EPS)
        return (
            floats * inverse * mod[scale_row : scale_row + 1, :] + mod[shift_row : shift_row + 1, :]
        ).astype(BF16)

    for i in (3, 5, 6):
        loads[i].wait()
    ctx_hidden[...] = normed(context[...], 1, 3)
    tile = tile_of(pair, 512)

    def ctx_project(j):
        at = pl.multiple_of(j * tile, tile)
        ctx_kv[sp, :, pl.ds(at, tile)] = jnp.dot(
            ctx_hidden[...], wk[:, pl.ds(at, tile)], preferred_element_type=F32
        ).astype(BF16)
        ctx_kv[sp, :, pl.ds(pl.multiple_of(pair + at, tile), tile)] = jnp.dot(
            ctx_hidden[...], wv[:, pl.ds(at, tile)], preferred_element_type=F32
        ).astype(BF16)

    loop(0, pair // tile, ctx_project)

    lines = n_sp // QUAD
    line, corner = sp // QUAD, lax.rem(sp, QUAD)

    across = corner + 1 - 2 * lax.rem(corner, 2)
    beside = lax.rem(corner + 2, QUAD)
    opposite = QUAD - 1 - corner

    def ctx_copy(slot, peer, sem, half=None):
        cols = slice(None) if half is None else pl.ds(half * pair, pair)
        return pltpu.make_async_remote_copy(
            src_ref=ctx_kv.at[slot, :, cols],
            dst_ref=ctx_kv.at[slot, :, cols],
            send_sem=ctx_send.at[sem],
            recv_sem=ctx_recv.at[slot, half or 0],
            device_id={"sp": peer},
            device_id_type=MESH,
        )

    ctx_sends = []

    def send_ctx(slot, peer, half=None):
        copy = ctx_copy(slot, peer, len(ctx_sends), half)
        copy.start()
        ctx_sends.append(copy)

    def send_quad(slot):
        send_ctx(slot, line * QUAD + across)
        send_ctx(slot, line * QUAD + beside)

    for d in range(1, lines):
        send_ctx(sp, lax.rem(line + d, lines) * QUAD + corner)
    send_quad(sp)

    def line_base(d):
        return lax.rem(line + lines - d, lines) * QUAD

    def forward(d):
        slot = line_base(d) + corner
        ctx_copy(slot, sp, 0).wait_recv()
        send_quad(slot)

    def relay(d):
        ctx_copy(line_base(d) + across, sp, 0).wait_recv()
        send_ctx(line_base(d) + across, line * QUAD + beside, 0)
        ctx_copy(line_base(d) + beside, sp, 0).wait_recv()
        send_ctx(line_base(d) + beside, line * QUAD + across, 1)

    gather_steps = []
    for d in range(lines):
        if d + 1 < lines:
            gather_steps.append(functools.partial(forward, d + 1))
        gather_steps.append(functools.partial(relay, d))

    def serve(count):
        for step in gather_steps[:count]:
            step()
        del gather_steps[:count]

    own_start = pl.multiple_of(WINDOW_REACH + tp * rows, strip)

    def norm_strip(i):
        at = pl.multiple_of(i * strip, strip)
        hidden[pl.ds(pl.multiple_of(own_start + at, strip), strip), :] = (
            own_total[pl.ds(at, strip), :] * mod[2:3, :] + mod[0:1, :]
        ).astype(BF16)

    loop(0, rows // strip, norm_strip)

    def hid_copy(d, mine):
        peer = lax.rem(tp + d, n_tp)
        slot = tp if mine else peer
        at = pl.multiple_of(WINDOW_REACH + slot * rows, strip)
        mine_at = pl.multiple_of(WINDOW_REACH + tp * rows, strip)
        return pltpu.make_async_remote_copy(
            src_ref=hidden.at[pl.ds(mine_at, rows)],
            dst_ref=hidden.at[pl.ds(at, rows)],
            send_sem=hid_send.at[peer],
            recv_sem=hid_recv.at[slot],
            device_id={"tp": peer},
            device_id_type=MESH,
        )

    loop(1, n_tp, lambda d: hid_copy(d, True).start())

    quarter = HEAD_DIM // 4
    def turned(values, cosine, sine):
        pieces = []
        lane = lax.broadcasted_iota(jnp.int32, cosine.shape, 1)
        low_half = lax.rem(lane, 2 * quarter) < quarter
        for h in range(values.shape[1] // HEAD_DIM):
            u = values[:, h * HEAD_DIM : (h + 1) * HEAD_DIM]
            other = jnp.where(
                low_half, pltpu.roll(u, HEAD_DIM - quarter, 1), pltpu.roll(u, quarter, 1)
            )
            pieces.append(u * cosine + other * sine)
        return jnp.concatenate(pieces, axis=1).astype(BF16)

    aligned = rows % WINDOW_REACH == 0

    def project_kv(start):
        source = pl.ds(pl.multiple_of(start, strip), rows)

        def one(j):
            col = pl.multiple_of(j * tile, tile)
            keys = jnp.dot(hidden[source, :], wk[:, pl.ds(col, tile)], preferred_element_type=F32)
            keys_kept[source, pl.ds(col, tile)] = turned(keys, cos_ref[source, :], sin_ref[source, :])
            values = jnp.dot(hidden[source, :], wv[:, pl.ds(col, tile)], preferred_element_type=F32)
            if aligned:
                at = pl.ds(pl.multiple_of(start, WINDOW_REACH), rows)
                values_t[pl.ds(col, tile), at] = values.astype(BF16).T
            else:
                values_kept[source, pl.ds(col, tile)] = values.astype(BF16)

        loop(0, pair // tile, one)

    def transpose_values():
        if not aligned:

            def one(i):
                at = pl.ds(pl.multiple_of(WINDOW_REACH * (i + 1), WINDOW_REACH), WINDOW_REACH)
                values_t[:, at] = values_kept[at, :].T

            loop(0, group_rows // WINDOW_REACH, one)

    def project_q(slot, begin=0, end=None):
        target = pl.ds(pl.multiple_of(slot * rows, strip), rows)
        source = pl.ds(pl.multiple_of(WINDOW_REACH + slot * rows, strip), rows)
        q_tile = tile_of(query_width, 512)

        def one(j):
            col = pl.multiple_of(j * q_tile, q_tile)
            q = jnp.dot(hidden[source, :], wq[:, pl.ds(col, q_tile)], preferred_element_type=F32)
            queries[target, pl.ds(col, q_tile)] = turned(
                q * factor, cos_ref[source, :], sin_ref[source, :]
            )

        count = query_width // q_tile
        loop(begin * count // 2, (2 if end is None else end) * count // 2, one)

    log2e = 1.4426950408889634
    factor = HEAD_DIM ** (-0.5) * log2e
    def halo_copies(up):
        source = group_rows if up else WINDOW_REACH
        target = 0 if up else group_rows + WINDOW_REACH
        which = 0 if up else 1
        peer = {"sp": lax.rem(sp + (1 if up else n_sp - 1), n_sp)}
        ends = (
            (keys_kept.at[pl.ds(source, WINDOW_REACH)], keys_kept.at[pl.ds(target, WINDOW_REACH)]),
            (
                values_t.at[:, pl.ds(source, WINDOW_REACH)],
                values_t.at[:, pl.ds(target, WINDOW_REACH)],
            ),
        )
        return [
            pltpu.make_async_remote_copy(
                src_ref=src,
                dst_ref=dst,
                send_sem=halo_send.at[which, i],
                recv_sem=halo_recv.at[which, i],
                device_id=peer,
                device_id_type=MESH,
            )
            for i, (src, dst) in enumerate(ends)
        ]

    def send_halo():
        if raw_halo:
            return

        @pl.when(has_next)
        def _():
            for copy in halo_copies(True):
                copy.start()

        @pl.when(has_last)
        def _():
            for copy in halo_copies(False):
                copy.start()

        def clear(at):
            region = pl.ds(at, WINDOW_REACH)
            keys_kept[region, :] = jnp.zeros((WINDOW_REACH, pair), BF16)
            values_t[:, region] = jnp.zeros((pair, WINDOW_REACH), BF16)

        @pl.when(jnp.logical_not(has_last))
        def _():
            clear(0)

        @pl.when(jnp.logical_not(has_next))
        def _():
            clear(group_rows + WINDOW_REACH)

    def edge_copy(low, d, mine):
        peer = lax.rem(tp + d, n_tp) if mine else tp
        which = 0 if low else 1
        region = pl.ds(which * WINDOW_REACH, WINDOW_REACH)
        return pltpu.make_async_remote_copy(
            src_ref=edge_hidden.at[region],
            dst_ref=edge_hidden.at[region],
            send_sem=edge_send.at[which, peer],
            recv_sem=edge_recv.at[which],
            device_id={"tp": peer},
            device_id_type=MESH,
        )

    def scale_edge(low):
        which = 0 if low else 1
        raw_copy(low, 0).wait_recv()
        raw_copy(low, 1).wait_recv()

        def one(i):
            at = pl.multiple_of(i * strip, strip)
            edge_hidden[pl.ds(which * WINDOW_REACH + at, strip), :] = normed(
                halo_raw[which, pl.ds(at, strip), :], 0, 2
            )

        loop(0, WINDOW_REACH // strip, one)
        loop(1, n_tp, lambda d: edge_copy(low, d, True).start())

    def scale_edges():
        if not raw_halo:
            return

        @pl.when(has_last & holds_last)
        def _():
            scale_edge(True)

        @pl.when(has_next & holds_first)
        def _():
            scale_edge(False)

        @pl.when(jnp.logical_not(has_last))
        def _():
            edge_hidden[:WINDOW_REACH, :] = jnp.zeros((WINDOW_REACH, width), BF16)

        @pl.when(jnp.logical_not(has_next))
        def _():
            edge_hidden[WINDOW_REACH:, :] = jnp.zeros((WINDOW_REACH, width), BF16)

    def project_edges():
        if not raw_halo:
            return

        @pl.when(has_last & jnp.logical_not(holds_last))
        def _():
            edge_copy(True, 0, False).wait_recv()

        @pl.when(has_next & jnp.logical_not(holds_first))
        def _():
            edge_copy(False, 0, False).wait_recv()

        def one(j):
            col = pl.multiple_of(j * tile, tile)
            keys = jnp.dot(edge_hidden[...], wk[:, pl.ds(col, tile)], preferred_element_type=F32)
            values = jnp.dot(edge_hidden[...], wv[:, pl.ds(col, tile)], preferred_element_type=F32)
            for which, start in enumerate((0, WINDOW_REACH + group_rows)):
                part = slice(which * WINDOW_REACH, (which + 1) * WINDOW_REACH)
                at = pl.ds(start, WINDOW_REACH)
                keys_kept[at, pl.ds(col, tile)] = turned(keys[part], cos_ref[at, :], sin_ref[at, :])
                values_t[pl.ds(col, tile), at] = values[part].astype(BF16).T

        loop(0, pair // tile, one)

    def receive_halo():
        if raw_halo:
            return

        @pl.when(has_last)
        def _():
            for copy in halo_copies(True):
                copy.wait_recv()

        @pl.when(has_next)
        def _():
            for copy in halo_copies(False):
                copy.wait_recv()

    span = 3 * WINDOW_REACH
    stacked = per_group * WINDOW_REACH
    contract = (((1,), (1,)), ((), ()))
    blocks = group_rows // WINDOW_REACH
    lines_each = max(1, 256 // (QUAD * ctx_rows))
    ctx_chunks = lines // lines_each
    slots_each = QUAD * lines_each
    chunk_rows = slots_each * ctx_rows
    ahead = lax.rem(
        lax.broadcasted_iota(jnp.int32, (WINDOW_REACH, stacked), 1), WINDOW_REACH
    ) - lax.broadcasted_iota(jnp.int32, (WINDOW_REACH, stacked), 0)
    WINDOW = "window"

    def chunk_at(k):
        return lax.rem(line // lines_each + ctx_chunks - k, ctx_chunks)

    def query_heads(h):
        return range(h * per_group, (h + 1) * per_group)

    def scores(block, h, piece):
        begin = pl.multiple_of(block * WINDOW_REACH, WINDOW_REACH)
        cols = slice(h * HEAD_DIM, (h + 1) * HEAD_DIM)
        q = jnp.concatenate(
            [
                queries[pl.ds(begin, WINDOW_REACH), i * HEAD_DIM : (i + 1) * HEAD_DIM]
                for i in query_heads(h)
            ],
            axis=0,
        )
        if piece is not WINDOW:
            keys = ctx_kv[pl.ds(piece * slots_each, slots_each), :, cols]
            keys = keys.reshape(chunk_rows, HEAD_DIM)
            return lax.dot_general(keys, q, contract, preferred_element_type=F32)
        keys = keys_kept[pl.ds(begin, span), cols]
        band = lax.dot_general(keys, q, contract, preferred_element_type=F32)
        lowest = jnp.where((block > 0) | has_last, 0, -span)
        highest = jnp.where((block < blocks - 1) | has_next, 0, span)
        return jnp.concatenate(
            [
                jnp.where(ahead <= lowest, band[:WINDOW_REACH], MASKED_SCORE),
                band[WINDOW_REACH : 2 * WINDOW_REACH],
                jnp.where(ahead >= highest, band[2 * WINDOW_REACH :], MASKED_SCORE),
            ],
            axis=0,
        )

    def weighted(block, h, piece, probs):
        cols = slice(h * HEAD_DIM, (h + 1) * HEAD_DIM)
        if piece is WINDOW:
            begin = pl.multiple_of(block * WINDOW_REACH, WINDOW_REACH)
            values = values_t[cols, pl.ds(begin, span)]
        else:
            begin = pl.multiple_of(piece * chunk_rows, chunk_rows)
            values = ctx_values_t[cols, pl.ds(begin, chunk_rows)]
        ones = jnp.ones((16, probs.shape[0]), BF16)
        return jnp.dot(
            jnp.concatenate([values, ones], axis=0), probs, preferred_element_type=F32
        )[: HEAD_DIM + 8]

    def sinks(h):
        return jnp.concatenate(
            [jnp.full((1, WINDOW_REACH), sink_ref[0, i] * log2e, F32) for i in query_heads(h)],
            axis=1,
        )

    def attend(items, first=False, last=False):
        tasks = [(b, h, pieces) for b, pieces in items for h in range(kv_local)]
        top, total = {}, {}
        following = {i: scores(b, h, pieces[0]) for i, (b, h, pieces) in enumerate(tasks)}
        for step in range(max(len(pieces) for _, pieces in items)):
            current, following, now = following, {}, {}
            live = [(i, *task) for i, task in enumerate(tasks) if step < len(task[2])]
            for i, b, h, pieces in live:
                if step + 1 < len(pieces):
                    following[i] = scores(b, h, pieces[step + 1])
            for i, b, h, pieces in live:
                if step == 0:
                    top[i] = sinks(h) if first else tops[b, h, 0:1, :]
                now[i] = jnp.maximum(top[i], jnp.max(current[i], axis=0, keepdims=True))
            probs = {i: jnp.exp2(current[i] - now[i]).astype(BF16) for i, *_ in live}
            for i, b, h, pieces in live:
                added = weighted(b, h, pieces[step], probs[i])
                shrink = jnp.exp2(top[i] - now[i])
                if step == 0 and first:
                    total[i] = jnp.concatenate(
                        [added[:HEAD_DIM], added[HEAD_DIM:] + shrink], axis=0
                    )
                else:
                    total[i] = (sums[b, h] if step == 0 else total[i]) * shrink + added
                top[i] = now[i]
        for i, (b, h, pieces) in enumerate(tasks):
            if last:
                mixed = total[i][:HEAD_DIM] / total[i][HEAD_DIM : HEAD_DIM + 1]
                mixed = mixed.T.astype(BF16)
                here = pl.ds(pl.multiple_of(b * WINDOW_REACH, WINDOW_REACH), WINDOW_REACH)
                for n, k in enumerate(query_heads(h)):
                    attended[here, k * HEAD_DIM : (k + 1) * HEAD_DIM] = mixed[
                        n * WINDOW_REACH : (n + 1) * WINDOW_REACH
                    ]
            else:
                sums[b, h] = total[i]
                tops[b, h, 0:1, :] = top[i]

    def attend_all(n, first_block, pieces, most, **kind):
        each = max(i for i in range(1, most + 1) if n % i == 0)
        loop(
            0,
            n // each,
            lambda g: attend([(first_block + g * each + i, pieces) for i in range(each)], **kind),
        )

    def start_block(b):
        for h in range(kv_local):
            sums[b, h, :HEAD_DIM, :] = jnp.zeros((HEAD_DIM, stacked), F32)
            sums[b, h, HEAD_DIM:, :] = jnp.ones((8, stacked), F32)
            tops[b, h, 0:1, :] = sinks(h)

    def opposite_arrived(base):
        for half in range(2):
            ctx_copy(base + opposite, sp, 0, half).wait_recv()

    def transpose_chunk(piece):
        values = ctx_kv[pl.ds(piece * slots_each, slots_each), :, pl.ds(pair, pair)]
        at = pl.multiple_of(piece * chunk_rows, chunk_rows)
        ctx_values_t[:, pl.ds(at, chunk_rows)] = values.reshape(chunk_rows, pair).T

    def receive_chunk(k):
        if lines_each == 1:
            opposite_arrived(line_base(k))
        elif k == 0:
            loop(0, lines, lambda i: opposite_arrived(i * QUAD))
        transpose_chunk(chunk_at(k))

    early = aligned and n_tp == 2 and blocks >= 6
    inner = blocks - 2

    loads[7].wait()
    project_kv(WINDOW_REACH + tp * rows)
    project_q(tp)
    loop(1, n_tp, lambda d: hid_copy(d, False).wait_recv())
    serve(2)
    loop(1, n_tp, lambda d: project_kv(WINDOW_REACH + lax.rem(tp + d, n_tp) * rows))
    transpose_values()
    send_halo()
    if early:
        project_q(1 - tp, 0, 1)
        serve(1)
        project_q(1 - tp, 1, 2)
        serve(1)
        attend_all(inner, 1, [WINDOW], 2, first=True)
        start_block(0)
        start_block(blocks - 1)
        serve(2)
    else:
        loop(1, n_tp, lambda d: project_q(lax.rem(tp + d, n_tp)))
        loop(0, blocks, start_block)
    if lines_each > 1:
        serve(len(gather_steps))
    receive_chunk(0)
    attend_all(blocks, 0, [chunk_at(0)], 3)
    serve(len(gather_steps))
    scale_edges()
    for k in range(1, ctx_chunks - 1):
        receive_chunk(k)
        attend_all(blocks, 0, [chunk_at(k)], 3)
    project_edges()
    receive_chunk(ctx_chunks - 1)
    receive_halo()
    final = chunk_at(ctx_chunks - 1)

    part_blocks = rows // WINDOW_REACH

    def finish_part(slot):
        if early:
            edge = slot * (blocks - 1)
            from_block = slot * part_blocks + 1 - slot
            inside = [(from_block + i, [final]) for i in range(part_blocks - 1)]
            attend(inside + [(edge, [final, WINDOW])], last=True)

    if not early:
        attend_all(blocks, 0, [final, WINDOW], 2, last=True)
    loads[8].wait()
    out_tile = tile_of(width, 512)

    def out_copy(d, mine):
        peer = lax.rem(tp + d, n_tp)
        slot = tp if mine else peer
        return pltpu.make_async_remote_copy(
            src_ref=partial_out.at[peer],
            dst_ref=partial_in.at[slot],
            send_sem=out_send.at[peer],
            recv_sem=out_recv.at[slot],
            device_id={"tp": peer},
            device_id_type=MESH,
        )

    def project_out(slot, store):
        source = pl.ds(pl.multiple_of(slot * rows, strip), rows)

        def one(j):
            cols = pl.ds(pl.multiple_of(j * out_tile, out_tile), out_tile)
            store(
                cols,
                jnp.dot(attended[source, :], wo[:, cols], preferred_element_type=F32).astype(BF16),
            )

        loop(0, width // out_tile, one)

    def peer_part(d):
        slot = lax.rem(tp + d, n_tp)
        finish_part(slot)

        def store(cols, value):
            partial_out[slot, :, cols] = value

        project_out(slot, store)
        out_copy(d, True).start()

    loop(1, n_tp, peer_part)
    finish_part(tp)

    def keep(cols, value):
        own_total[:, cols] = value.astype(F32)

    project_out(tp, keep)
    loop(1, n_tp, lambda d: out_copy(d, False).wait_recv())

    def finish(i):
        at = pl.ds(pl.multiple_of(i * strip, strip), strip)
        mixed = own_total[at, :]
        for d in range(1, n_tp):
            mixed = mixed + partial_in[lax.rem(tp + d, n_tp), at, :].astype(F32)
        out_ref[at, :] = (latent[at, :].astype(F32) + mod[4:5, :] * mixed).astype(BF16)

    loop(0, rows // strip, finish)

    loop(1, n_tp, lambda d: hid_copy(d, True).wait_send())
    loop(1, n_tp, lambda d: out_copy(d, True).wait_send())
    for copy in ctx_sends:
        copy.wait_send()

    if raw_halo:

        @pl.when(has_next & holds_last)
        def _():
            raw_copy(True, 0).wait_send()
            raw_copy(True, 1).wait_send()

        @pl.when(has_last & holds_first)
        def _():
            raw_copy(False, 0).wait_send()
            raw_copy(False, 1).wait_send()

        @pl.when(has_last & holds_last)
        def _():
            loop(1, n_tp, lambda d: edge_copy(True, d, True).wait_send())

        @pl.when(has_next & holds_first)
        def _():
            loop(1, n_tp, lambda d: edge_copy(False, d, True).wait_send())
    else:

        @pl.when(has_next)
        def _():
            for copy in halo_copies(True):
                copy.wait_send()

        @pl.when(has_last)
        def _():
            for copy in halo_copies(False):
                copy.wait_send()


def angle_tables(total_rows):
    inv_freq = np.power(
        10000.0, -np.arange(0, HEAD_DIM // 2, 2, dtype=np.float64) / (HEAD_DIM // 2)
    ).astype(np.float32)

    def tables(count):
        angle = (np.arange(count, dtype=np.float32)[:, None] * inv_freq).astype(np.float64)
        cosine, sine = np.cos(angle), np.sin(angle)
        return (
            np.concatenate([cosine, cosine], axis=1).astype(np.float32),
            np.concatenate([-sine, sine], axis=1).astype(np.float32),
        )

    empty = HEAD_DIM // 2
    by_row = [np.pad(t, ((0, 0), (0, empty))) for t in tables(total_rows // GRID_W)]
    by_col = [np.pad(t, ((0, 0), (empty, 0))) for t in tables(GRID_W)]
    return by_row + by_col


def shards(
    n_sp,
    n_tp,
    latent,
    condition,
    context_condition,
    context,
    norm_gain,
    shift_weight,
    scale_weight,
    gate_weight,
    query_weight,
    key_matrix,
    value_matrix,
    sink_logit_head,
    out_weight,
):
    rows, width = latent.shape
    group_rows = rows * n_tp
    angles = [jnp.asarray(t) for t in angle_tables(group_rows * n_sp)]
    columns = shift_weight.shape[1]
    groups = 5 * columns // LANES
    per = -(-groups // n_sp)
    query_width = query_weight.shape[1]
    pair = key_matrix.shape[1]
    ctx_rows = context.shape[0]
    lines = n_sp // QUAD
    ctx_sends = (lines - 1) + 4 * lines
    padded = group_rows + 2 * WINDOW_REACH
    state = (group_rows // WINDOW_REACH, pair // HEAD_DIM)
    stacked = query_width // pair * WINDOW_REACH
    dma = pltpu.SemaphoreType.DMA
    vmem = pl.BlockSpec(memory_space=pltpu.VMEM)
    anywhere = pl.BlockSpec(memory_space=pl.ANY)

    def like(array):
        return pltpu.VMEM(array.shape, array.dtype)

    return pl.pallas_call(
        functools.partial(block_kernel, n_sp, n_tp),
        out_shape=jax.ShapeDtypeStruct((rows, width), BF16),
        in_specs=[vmem] * 7 + [pl.BlockSpec(memory_space=pltpu.SMEM)] + [anywhere] * 9,
        out_specs=vmem,
        scratch_shapes=[
            like(latent),
            like(context),
            like(shift_weight),
            like(scale_weight),
            like(gate_weight),
            like(query_weight),
            like(key_matrix),
            like(value_matrix),
            like(out_weight),
            pltpu.VMEM((n_sp, per, LANES), F32),
            pltpu.VMEM((n_sp, per, LANES), F32),
            pltpu.VMEM((n_tp, n_sp, per, LANES), F32),
            pltpu.VMEM((8, width), F32),
            pltpu.VMEM((padded, width), BF16),
            like(context),
            pltpu.VMEM((group_rows, query_width), BF16),
            pltpu.VMEM((padded, pair), BF16),
            pltpu.VMEM((8 if rows % WINDOW_REACH == 0 else padded, pair), BF16),
            pltpu.VMEM((pair, padded), BF16),
            pltpu.VMEM((n_sp, ctx_rows, 2 * pair), BF16),
            pltpu.VMEM((pair, n_sp * ctx_rows), BF16),
            pltpu.VMEM((*state, HEAD_DIM + 8, stacked), F32),
            pltpu.VMEM((*state, 8, stacked), F32),
            pltpu.VMEM((group_rows, query_width), BF16),
            pltpu.VMEM((n_tp, rows, width), BF16),
            pltpu.VMEM((n_tp, rows, width), BF16),
            pltpu.VMEM((rows, width), F32),
            pltpu.VMEM((group_rows + 2 * WINDOW_REACH, HEAD_DIM), F32),
            pltpu.VMEM((group_rows + 2 * WINDOW_REACH, HEAD_DIM), F32),
            pltpu.VMEM((2, WINDOW_REACH, width), BF16),
            pltpu.VMEM((2 * WINDOW_REACH, width), BF16),
            dma((9,)),
            dma((n_sp,)),
            dma((n_sp,)),
            dma((n_tp, n_sp)),
            dma((n_tp, n_sp)),
            dma((n_tp,)),
            dma((n_tp,)),
            dma((ctx_sends,)),
            dma((n_sp, 2)),
            dma((2, 2)),
            dma((2, 2)),
            dma((2, n_tp)),
            dma((2,)),
            dma((n_tp,)),
            dma((n_tp,)),
        ],
        compiler_params=pltpu.CompilerParams(
            collective_id=0, has_side_effects=True, vmem_limit_bytes=63 * 1024 * 1024
        ),
    )(
        condition.reshape(1, -1),
        context_condition.reshape(1, -1),
        norm_gain.reshape(1, -1),
        *angles,
        sink_logit_head.reshape(1, -1),
        latent,
        context,
        shift_weight,
        scale_weight,
        gate_weight,
        query_weight,
        key_matrix,
        value_matrix,
        out_weight,
    )


def solution(mesh):
    placed = (
        P(("sp", "tp"), None),
        P("sp"),
        P("sp"),
        P("sp", None),
        P(),
        P("sp", "tp"),
        P("sp", "tp"),
        P("sp", "tp"),
        P(None, "tp"),
        P(None, "tp"),
        P(None, "tp"),
        P("tp"),
        P("tp", None),
    )
    return jax.shard_map(
        functools.partial(shards, mesh.shape["sp"], mesh.shape["tp"]),
        mesh=mesh,
        in_specs=placed,
        out_specs=P(("sp", "tp"), None),
        check_vma=False,
    )
```

```python
import functools

import jax
import jax.numpy as jnp
import numpy as np
from jax import lax
from jax.experimental import pallas as pl
from jax.experimental.pallas import tpu as pltpu
from jax.sharding import PartitionSpec as P

QUERY_HEADS = 16
KEY_VALUE_HEADS = 8
HEAD_DIM = 128
WINDOW_REACH = 128
GRID_W = 64
NORM_EPS = 1e-05
MASKED_SCORE = -1e30
LANES = 128
QUAD = 4
MESH = pl.DeviceIdType.MESH
F32 = jnp.float32
BF16 = jnp.bfloat16


def tile_of(extent, most):
    tile = min(extent, most)
    while extent % tile:
        tile -= LANES
    return tile


def block_kernel(
    n_sp,
    n_tp,
    cond_ref,
    ctx_cond_ref,
    gain_ref,
    row_cos,
    row_sin,
    col_cos,
    col_sin,
    sink_ref,
    latent_hbm,
    context_hbm,
    shift_hbm,
    scale_hbm,
    gate_hbm,
    wq_hbm,
    wk_hbm,
    wv_hbm,
    wo_hbm,
    out_ref,
    latent,
    context,
    shift_w,
    scale_w,
    gate_w,
    wq,
    wk,
    wv,
    wo,
    part,
    line_parts,
    quad_parts,
    mod,
    hidden,
    ctx_hidden,
    queries,
    keys_kept,
    values_kept,
    values_t,
    ctx_kv,
    ctx_values_t,
    sums,
    tops,
    attended,
    partial_out,
    partial_in,
    own_total,
    cos_ref,
    sin_ref,
    halo_raw,
    edge_hidden,
    load_sem,
    line_send,
    line_recv,
    quad_send,
    quad_recv,
    hid_send,
    hid_recv,
    ctx_send,
    ctx_recv,
    halo_send,
    halo_recv,
    edge_send,
    edge_recv,
    out_send,
    out_recv,
):
    sp = lax.axis_index("sp")
    tp = lax.axis_index("tp")
    rows, width = latent.shape
    group_rows = rows * n_tp
    columns = shift_w.shape[1]
    chunks = columns // LANES
    query_width = wq.shape[1]
    pair = wk.shape[1]
    kv_local = pair // HEAD_DIM
    per_group = query_width // pair
    ctx_rows = context.shape[0]

    loads = [
        pltpu.make_async_copy(src, dst, load_sem.at[i])
        for i, (src, dst) in enumerate(
            [
                (shift_hbm, shift_w),
                (scale_hbm, scale_w),
                (gate_hbm, gate_w),
                (context_hbm, context),
                (latent_hbm, latent),
                (wk_hbm, wk),
                (wv_hbm, wv),
                (wq_hbm, wq),
                (wo_hbm, wo),
            ]
        )
    ]
    for load in loads:
        load.start()

    barrier = pltpu.get_barrier_semaphore()

    lines = n_sp // QUAD
    line, corner = sp // QUAD, lax.rem(sp, QUAD)
    cluster = QUAD * n_tp

    def loop(low, high, f):
        def step(i, carry):
            f(i)
            return carry

        lax.fori_loop(low, high, step, 0)

    def in_line(d):
        peer = lax.rem(line + d, lines)
        return peer, {"sp": peer * QUAD + corner}

    def in_cluster(d):
        at = lax.rem(corner * n_tp + tp + d, cluster)
        peer, peer_tp = at // n_tp, lax.rem(at, n_tp)
        return peer, peer_tp, {"sp": line * QUAD + peer, "tp": peer_tp}

    def greet(device):
        pl.semaphore_signal(barrier, inc=1, device_id=device, device_id_type=MESH)

    loop(1, lines, lambda d: greet(in_line(d)[1]))
    loop(1, cluster, lambda d: greet(in_cluster(d)[2]))
    for d in (1, n_sp - 1):
        greet({"sp": lax.rem(sp + d, n_sp)})

    def silu(v):
        return v / (1.0 + jnp.exp(-v))

    depth = cond_ref.shape[1]
    row_id = lax.broadcasted_iota(jnp.int32, (16, depth), 0)
    active = jnp.where(
        row_id == 0,
        jnp.broadcast_to(silu(cond_ref[...]), (16, depth)),
        jnp.broadcast_to(silu(ctx_cond_ref[...]), (16, depth)),
    ).astype(BF16)
    part[...] = jnp.zeros_like(part)
    vector = 0
    for load, weight, count in zip(loads[:3], (shift_w, scale_w, gate_w), (2, 2, 1)):
        load.wait()
        product = jnp.dot(active, weight[...], preferred_element_type=F32)
        for v in range(count):
            for j in range(chunks):
                g = vector * chunks + j
                part[g : g + 1, :] = product[
                    v : v + 1, j * LANES : (j + 1) * LANES
                ]
            vector += 1

    pl.semaphore_wait(barrier, lines + cluster)

    def line_copy(d, mine):
        peer, device = in_line(d)
        slot = line if mine else peer
        return pltpu.make_async_remote_copy(
            src_ref=part,
            dst_ref=line_parts.at[slot],
            send_sem=line_send.at[peer],
            recv_sem=line_recv.at[slot],
            device_id=device,
            device_id_type=MESH,
        )

    has_next, has_last = sp < n_sp - 1, sp > 0
    holds_last, holds_first = tp == n_tp - 1, tp == 0
    raw_halo = rows >= WINDOW_REACH
    raw_ends = (0, 0, 128, 128)

    def raw_copy(up, piece):
        which = 0 if up else 1
        base = rows - WINDOW_REACH if up else 0
        begin, count = raw_ends[piece], raw_ends[piece + 1] - raw_ends[piece]
        return pltpu.make_async_remote_copy(
            src_ref=latent.at[pl.ds(base + begin, count)],
            dst_ref=halo_raw.at[which, pl.ds(begin, count)],
            send_sem=halo_send.at[which, piece],
            recv_sem=halo_recv.at[which, piece],
            device_id={"sp": lax.rem(sp + (1 if up else n_sp - 1), n_sp)},
            device_id_type=MESH,
        )

    raw_pieces = [i for i in range(3) if raw_ends[i + 1] > raw_ends[i]]

    def send_raw(piece):
        if raw_halo and piece in raw_pieces:

            @pl.when(has_next & holds_last)
            def _():
                raw_copy(True, piece).start()

            @pl.when(has_last & holds_first)
            def _():
                raw_copy(False, piece).start()

    loop(1, lines, lambda d: line_copy(d, True).start())
    line_parts[line] = part[...]
    loads[4].wait()
    loop(1, lines, lambda d: line_copy(d, True).wait_send())
    send_raw(0)

    strip = 32

    def scale_strip(i):
        at = pl.multiple_of(i * strip, strip)
        floats = latent[pl.ds(at, strip), :].astype(F32)
        inverse = lax.rsqrt(jnp.mean(floats * floats, axis=-1, keepdims=True) + NORM_EPS)
        own_total[pl.ds(at, strip), :] = floats * inverse

    loop(0, rows // strip, scale_strip)

    grid_rows = group_rows // GRID_W
    grid_pad = WINDOW_REACH // GRID_W
    in_row = lax.broadcasted_iota(jnp.int32, (GRID_W, HEAD_DIM), 1) < HEAD_DIM // 2

    def fill_angles(i):
        row = jnp.clip(sp * grid_rows - grid_pad + i, 0, n_sp * grid_rows - 1)
        at = pl.ds(pl.multiple_of(i * GRID_W, GRID_W), GRID_W)
        for target, by_row, by_col in ((cos_ref, row_cos, col_cos), (sin_ref, row_sin, col_sin)):
            spread = jnp.broadcast_to(by_row[pl.ds(row, 1), :], (GRID_W, HEAD_DIM))
            target[at, :] = jnp.where(in_row, spread, by_col[...])

    loop(0, grid_rows + 2 * grid_pad, fill_angles)
    loop(1, lines, lambda d: line_copy(d, False).wait_recv())
    quad_parts[tp, corner] = jnp.sum(line_parts[...], axis=0)

    def quad_copy(d, mine):
        peer, peer_tp, device = in_cluster(d)
        at = (tp, corner) if mine else (peer_tp, peer)
        return pltpu.make_async_remote_copy(
            src_ref=quad_parts.at[tp, corner],
            dst_ref=quad_parts.at[at],
            send_sem=quad_send.at[peer_tp, peer],
            recv_sem=quad_recv.at[at],
            device_id=device,
            device_id_type=MESH,
        )

    loop(1, cluster, lambda d: quad_copy(d, True).start())
    loop(1, cluster, lambda d: quad_copy(d, True).wait_send())
    send_raw(1)
    loop(1, cluster, lambda d: quad_copy(d, False).wait_recv())
    for t in range(n_tp):
        whole = jnp.sum(quad_parts[t], axis=0)
        for v in range(5):
            for j in range(chunks):
                g = v * chunks + j
                column = t * columns + j * LANES
                mod[v : v + 1, column : column + LANES] = whole[g : g + 1, :]
    gain = gain_ref[...]
    mod[2:3, :] = gain * (1.0 + mod[2:3, :])
    mod[3:4, :] = gain * (1.0 + mod[3:4, :])

    def normed(block, shift_row, scale_row):
        floats = block.astype(F32)
        inverse = lax.rsqrt(jnp.mean(floats * floats, axis=-1, keepdims=True) + NORM_EPS)
        return (
            floats * inverse * mod[scale_row : scale_row + 1, :] + mod[shift_row : shift_row + 1, :]
        ).astype(BF16)

    for i in (3, 5, 6):
        loads[i].wait()
    ctx_hidden[...] = normed(context[...], 1, 3)
    tile = tile_of(pair, 512)

    def ctx_project(j):
        at = pl.multiple_of(j * tile, tile)
        ctx_kv[sp, :, pl.ds(at, tile)] = jnp.dot(
            ctx_hidden[...], wk[:, pl.ds(at, tile)], preferred_element_type=F32
        ).astype(BF16)
        ctx_kv[sp, :, pl.ds(pl.multiple_of(pair + at, tile), tile)] = jnp.dot(
            ctx_hidden[...], wv[:, pl.ds(at, tile)], preferred_element_type=F32
        ).astype(BF16)

    loop(0, pair // tile, ctx_project)

    across = corner + 1 - 2 * lax.rem(corner, 2)
    beside = lax.rem(corner + 2, QUAD)
    opposite = QUAD - 1 - corner

    def ctx_copy(slot, peer, sem, half=None):
        cols = slice(None) if half is None else pl.ds(half * pair, pair)
        return pltpu.make_async_remote_copy(
            src_ref=ctx_kv.at[slot, :, cols],
            dst_ref=ctx_kv.at[slot, :, cols],
            send_sem=ctx_send.at[sem],
            recv_sem=ctx_recv.at[slot, half or 0],
            device_id={"sp": peer},
            device_id_type=MESH,
        )

    ctx_sends = []

    def send_ctx(slot, peer, half=None):
        copy = ctx_copy(slot, peer, len(ctx_sends), half)
        copy.start()
        ctx_sends.append(copy)

    def send_quad(slot):
        send_ctx(slot, line * QUAD + across)
        send_ctx(slot, line * QUAD + beside)

    for d in range(1, lines):
        send_ctx(sp, lax.rem(line + d, lines) * QUAD + corner)
    send_quad(sp)
    send_raw(2)

    def line_base(d):
        return lax.rem(line + lines - d, lines) * QUAD

    def forward(d):
        slot = line_base(d) + corner
        ctx_copy(slot, sp, 0).wait_recv()
        send_quad(slot)

    def relay(d):
        ctx_copy(line_base(d) + across, sp, 0).wait_recv()
        send_ctx(line_base(d) + across, line * QUAD + beside, 0)
        ctx_copy(line_base(d) + beside, sp, 0).wait_recv()
        send_ctx(line_base(d) + beside, line * QUAD + across, 1)

    gather_steps = []
    for d in range(lines):
        if d + 1 < lines:
            gather_steps.append(functools.partial(forward, d + 1))
        gather_steps.append(functools.partial(relay, d))

    def serve(count):
        for step in gather_steps[:count]:
            step()
        del gather_steps[:count]

    own_start = pl.multiple_of(WINDOW_REACH + tp * rows, strip)

    def norm_strip(i):
        at = pl.multiple_of(i * strip, strip)
        hidden[pl.ds(pl.multiple_of(own_start + at, strip), strip), :] = (
            own_total[pl.ds(at, strip), :] * mod[2:3, :] + mod[0:1, :]
        ).astype(BF16)

    loop(0, rows // strip, norm_strip)

    def hid_copy(d, mine):
        peer = lax.rem(tp + d, n_tp)
        slot = tp if mine else peer
        at = pl.multiple_of(WINDOW_REACH + slot * rows, strip)
        mine_at = pl.multiple_of(WINDOW_REACH + tp * rows, strip)
        return pltpu.make_async_remote_copy(
            src_ref=hidden.at[pl.ds(mine_at, rows)],
            dst_ref=hidden.at[pl.ds(at, rows)],
            send_sem=hid_send.at[peer],
            recv_sem=hid_recv.at[slot],
            device_id={"tp": peer},
            device_id_type=MESH,
        )

    loop(1, n_tp, lambda d: hid_copy(d, True).start())

    quarter = HEAD_DIM // 4
    def turned(values, cosine, sine):
        pieces = []
        lane = lax.broadcasted_iota(jnp.int32, cosine.shape, 1)
        low_half = lax.rem(lane, 2 * quarter) < quarter
        for h in range(values.shape[1] // HEAD_DIM):
            u = values[:, h * HEAD_DIM : (h + 1) * HEAD_DIM]
            other = jnp.where(
                low_half, pltpu.roll(u, HEAD_DIM - quarter, 1), pltpu.roll(u, quarter, 1)
            )
            pieces.append(u * cosine + other * sine)
        return jnp.concatenate(pieces, axis=1).astype(BF16)

    aligned = rows % WINDOW_REACH == 0

    def project_kv(start):
        source = pl.ds(pl.multiple_of(start, strip), rows)

        def one(j):
            col = pl.multiple_of(j * tile, tile)
            keys = jnp.dot(hidden[source, :], wk[:, pl.ds(col, tile)], preferred_element_type=F32)
            keys_kept[source, pl.ds(col, tile)] = turned(keys, cos_ref[source, :], sin_ref[source, :])
            values = jnp.dot(hidden[source, :], wv[:, pl.ds(col, tile)], preferred_element_type=F32)
            if aligned:
                at = pl.ds(pl.multiple_of(start, WINDOW_REACH), rows)
                values_t[pl.ds(col, tile), at] = values.astype(BF16).T
            else:
                values_kept[source, pl.ds(col, tile)] = values.astype(BF16)

        loop(0, pair // tile, one)

    def transpose_values():
        if not aligned:

            def one(i):
                at = pl.ds(pl.multiple_of(WINDOW_REACH * (i + 1), WINDOW_REACH), WINDOW_REACH)
                values_t[:, at] = values_kept[at, :].T

            loop(0, group_rows // WINDOW_REACH, one)

    def project_q(slot, begin=0, end=None):
        target = pl.ds(pl.multiple_of(slot * rows, strip), rows)
        source = pl.ds(pl.multiple_of(WINDOW_REACH + slot * rows, strip), rows)
        q_tile = tile_of(query_width, 512)

        def one(j):
            col = pl.multiple_of(j * q_tile, q_tile)
            q = jnp.dot(hidden[source, :], wq[:, pl.ds(col, q_tile)], preferred_element_type=F32)
            queries[target, pl.ds(col, q_tile)] = turned(
                q * factor, cos_ref[source, :], sin_ref[source, :]
            )

        count = query_width // q_tile
        loop(begin * count // 2, (2 if end is None else end) * count // 2, one)

    log2e = 1.4426950408889634
    factor = HEAD_DIM ** (-0.5) * log2e
    def halo_copies(up):
        source = group_rows if up else WINDOW_REACH
        target = 0 if up else group_rows + WINDOW_REACH
        which = 0 if up else 1
        peer = {"sp": lax.rem(sp + (1 if up else n_sp - 1), n_sp)}
        ends = (
            (keys_kept.at[pl.ds(source, WINDOW_REACH)], keys_kept.at[pl.ds(target, WINDOW_REACH)]),
            (
                values_t.at[:, pl.ds(source, WINDOW_REACH)],
                values_t.at[:, pl.ds(target, WINDOW_REACH)],
            ),
        )
        return [
            pltpu.make_async_remote_copy(
                src_ref=src,
                dst_ref=dst,
                send_sem=halo_send.at[which, i],
                recv_sem=halo_recv.at[which, i],
                device_id=peer,
                device_id_type=MESH,
            )
            for i, (src, dst) in enumerate(ends)
        ]

    def send_halo():
        if raw_halo:
            return

        @pl.when(has_next)
        def _():
            for copy in halo_copies(True):
                copy.start()

        @pl.when(has_last)
        def _():
            for copy in halo_copies(False):
                copy.start()

        def clear(at):
            region = pl.ds(at, WINDOW_REACH)
            keys_kept[region, :] = jnp.zeros((WINDOW_REACH, pair), BF16)
            values_t[:, region] = jnp.zeros((pair, WINDOW_REACH), BF16)

        @pl.when(jnp.logical_not(has_last))
        def _():
            clear(0)

        @pl.when(jnp.logical_not(has_next))
        def _():
            clear(group_rows + WINDOW_REACH)

    def edge_copy(low, d, mine):
        peer = lax.rem(tp + d, n_tp) if mine else tp
        which = 0 if low else 1
        region = pl.ds(which * WINDOW_REACH, WINDOW_REACH)
        return pltpu.make_async_remote_copy(
            src_ref=edge_hidden.at[region],
            dst_ref=edge_hidden.at[region],
            send_sem=edge_send.at[which, peer],
            recv_sem=edge_recv.at[which],
            device_id={"tp": peer},
            device_id_type=MESH,
        )

    def scale_edge(low):
        which = 0 if low else 1
        for piece in raw_pieces:
            raw_copy(low, piece).wait_recv()

        def one(i):
            at = pl.multiple_of(i * strip, strip)
            edge_hidden[pl.ds(which * WINDOW_REACH + at, strip), :] = normed(
                halo_raw[which, pl.ds(at, strip), :], 0, 2
            )

        loop(0, WINDOW_REACH // strip, one)
        loop(1, n_tp, lambda d: edge_copy(low, d, True).start())

    def scale_edges():
        if not raw_halo:
            return

        @pl.when(has_last & holds_last)
        def _():
            scale_edge(True)

        @pl.when(has_next & holds_first)
        def _():
            scale_edge(False)

        @pl.when(jnp.logical_not(has_last))
        def _():
            edge_hidden[:WINDOW_REACH, :] = jnp.zeros((WINDOW_REACH, width), BF16)

        @pl.when(jnp.logical_not(has_next))
        def _():
            edge_hidden[WINDOW_REACH:, :] = jnp.zeros((WINDOW_REACH, width), BF16)

    def project_edges():
        if not raw_halo:
            return

        @pl.when(has_last & jnp.logical_not(holds_last))
        def _():
            edge_copy(True, 0, False).wait_recv()

        @pl.when(has_next & jnp.logical_not(holds_first))
        def _():
            edge_copy(False, 0, False).wait_recv()

        def one(j):
            col = pl.multiple_of(j * tile, tile)
            keys = jnp.dot(edge_hidden[...], wk[:, pl.ds(col, tile)], preferred_element_type=F32)
            values = jnp.dot(edge_hidden[...], wv[:, pl.ds(col, tile)], preferred_element_type=F32)
            for which, start in enumerate((0, WINDOW_REACH + group_rows)):
                part = slice(which * WINDOW_REACH, (which + 1) * WINDOW_REACH)
                at = pl.ds(start, WINDOW_REACH)
                keys_kept[at, pl.ds(col, tile)] = turned(keys[part], cos_ref[at, :], sin_ref[at, :])
                values_t[pl.ds(col, tile), at] = values[part].astype(BF16).T

        loop(0, pair // tile, one)

    def receive_halo():
        if raw_halo:
            return

        @pl.when(has_last)
        def _():
            for copy in halo_copies(True):
                copy.wait_recv()

        @pl.when(has_next)
        def _():
            for copy in halo_copies(False):
                copy.wait_recv()

    span = 3 * WINDOW_REACH
    stacked = per_group * WINDOW_REACH
    contract = (((1,), (1,)), ((), ()))
    blocks = group_rows // WINDOW_REACH
    lines_each = max(1, 256 // (QUAD * ctx_rows))
    ctx_chunks = lines // lines_each
    slots_each = QUAD * lines_each
    chunk_rows = slots_each * ctx_rows
    ahead = lax.rem(
        lax.broadcasted_iota(jnp.int32, (WINDOW_REACH, stacked), 1), WINDOW_REACH
    ) - lax.broadcasted_iota(jnp.int32, (WINDOW_REACH, stacked), 0)
    WINDOW = "window"

    def chunk_at(k):
        return lax.rem(line // lines_each + ctx_chunks - k, ctx_chunks)

    def query_heads(h):
        return range(h * per_group, (h + 1) * per_group)

    def scores(block, h, piece):
        begin = pl.multiple_of(block * WINDOW_REACH, WINDOW_REACH)
        cols = slice(h * HEAD_DIM, (h + 1) * HEAD_DIM)
        q = jnp.concatenate(
            [
                queries[pl.ds(begin, WINDOW_REACH), i * HEAD_DIM : (i + 1) * HEAD_DIM]
                for i in query_heads(h)
            ],
            axis=0,
        )
        if piece is not WINDOW:
            keys = ctx_kv[pl.ds(piece * slots_each, slots_each), :, cols]
            keys = keys.reshape(chunk_rows, HEAD_DIM)
            return lax.dot_general(keys, q, contract, preferred_element_type=F32)
        keys = keys_kept[pl.ds(begin, span), cols]
        band = lax.dot_general(keys, q, contract, preferred_element_type=F32)
        lowest = jnp.where((block > 0) | has_last, 0, -span)
        highest = jnp.where((block < blocks - 1) | has_next, 0, span)
        return jnp.concatenate(
            [
                jnp.where(ahead <= lowest, band[:WINDOW_REACH], MASKED_SCORE),
                band[WINDOW_REACH : 2 * WINDOW_REACH],
                jnp.where(ahead >= highest, band[2 * WINDOW_REACH :], MASKED_SCORE),
            ],
            axis=0,
        )

    def weighted(block, h, piece, probs):
        cols = slice(h * HEAD_DIM, (h + 1) * HEAD_DIM)
        if piece is WINDOW:
            begin = pl.multiple_of(block * WINDOW_REACH, WINDOW_REACH)
            values = values_t[cols, pl.ds(begin, span)]
        else:
            begin = pl.multiple_of(piece * chunk_rows, chunk_rows)
            values = ctx_values_t[cols, pl.ds(begin, chunk_rows)]
        ones = jnp.ones((16, probs.shape[0]), BF16)
        return jnp.dot(
            jnp.concatenate([values, ones], axis=0), probs, preferred_element_type=F32
        )[: HEAD_DIM + 8]

    def sinks(h):
        return jnp.concatenate(
            [jnp.full((1, WINDOW_REACH), sink_ref[0, i] * log2e, F32) for i in query_heads(h)],
            axis=1,
        )

    def attend(items, first=False, last=False):
        tasks = [(b, h, pieces) for b, pieces in items for h in range(kv_local)]
        top, total = {}, {}
        following = {i: scores(b, h, pieces[0]) for i, (b, h, pieces) in enumerate(tasks)}
        for step in range(max(len(pieces) for _, pieces in items)):
            current, following, now = following, {}, {}
            live = [(i, *task) for i, task in enumerate(tasks) if step < len(task[2])]
            for i, b, h, pieces in live:
                if step + 1 < len(pieces):
                    following[i] = scores(b, h, pieces[step + 1])
            for i, b, h, pieces in live:
                if step == 0:
                    top[i] = sinks(h) if first else tops[b, h, 0:1, :]
                now[i] = jnp.maximum(top[i], jnp.max(current[i], axis=0, keepdims=True))
            probs = {i: jnp.exp2(current[i] - now[i]).astype(BF16) for i, *_ in live}
            for i, b, h, pieces in live:
                added = weighted(b, h, pieces[step], probs[i])
                shrink = jnp.exp2(top[i] - now[i])
                if step == 0 and first:
                    total[i] = jnp.concatenate(
                        [added[:HEAD_DIM], added[HEAD_DIM:] + shrink], axis=0
                    )
                else:
                    total[i] = (sums[b, h] if step == 0 else total[i]) * shrink + added
                top[i] = now[i]
        for i, (b, h, pieces) in enumerate(tasks):
            if last:
                mixed = total[i][:HEAD_DIM] / total[i][HEAD_DIM : HEAD_DIM + 1]
                mixed = mixed.T.astype(BF16)
                here = pl.ds(pl.multiple_of(b * WINDOW_REACH, WINDOW_REACH), WINDOW_REACH)
                for n, k in enumerate(query_heads(h)):
                    attended[here, k * HEAD_DIM : (k + 1) * HEAD_DIM] = mixed[
                        n * WINDOW_REACH : (n + 1) * WINDOW_REACH
                    ]
            else:
                sums[b, h] = total[i]
                tops[b, h, 0:1, :] = top[i]

    def attend_all(n, first_block, pieces, most, **kind):
        each = max(i for i in range(1, most + 1) if n % i == 0)
        loop(
            0,
            n // each,
            lambda g: attend([(first_block + g * each + i, pieces) for i in range(each)], **kind),
        )

    def start_block(b):
        for h in range(kv_local):
            sums[b, h, :HEAD_DIM, :] = jnp.zeros((HEAD_DIM, stacked), F32)
            sums[b, h, HEAD_DIM:, :] = jnp.ones((8, stacked), F32)
            tops[b, h, 0:1, :] = sinks(h)

    def opposite_arrived(base):
        for half in range(2):
            ctx_copy(base + opposite, sp, 0, half).wait_recv()

    def transpose_chunk(piece):
        values = ctx_kv[pl.ds(piece * slots_each, slots_each), :, pl.ds(pair, pair)]
        at = pl.multiple_of(piece * chunk_rows, chunk_rows)
        ctx_values_t[:, pl.ds(at, chunk_rows)] = values.reshape(chunk_rows, pair).T

    def receive_chunk(k):
        if lines_each == 1:
            opposite_arrived(line_base(k))
        elif k == 0:
            loop(0, lines, lambda i: opposite_arrived(i * QUAD))
        transpose_chunk(chunk_at(k))

    early = aligned and n_tp == 2 and blocks >= 6
    inner = blocks - 2

    loads[7].wait()
    project_kv(WINDOW_REACH + tp * rows)
    project_q(tp)
    loop(1, n_tp, lambda d: hid_copy(d, False).wait_recv())
    serve(2)
    loop(1, n_tp, lambda d: project_kv(WINDOW_REACH + lax.rem(tp + d, n_tp) * rows))
    transpose_values()
    send_halo()
    if early:
        project_q(1 - tp, 0, 1)
        serve(1)
        project_q(1 - tp, 1, 2)
        serve(1)
        attend_all(inner, 1, [WINDOW], 2, first=True)
        start_block(0)
        start_block(blocks - 1)
        serve(2)
    else:
        loop(1, n_tp, lambda d: project_q(lax.rem(tp + d, n_tp)))
        loop(0, blocks, start_block)
    if lines_each > 1:
        serve(len(gather_steps))
    receive_chunk(0)
    attend_all(blocks, 0, [chunk_at(0)], 3)
    serve(len(gather_steps))
    scale_edges()
    for k in range(1, ctx_chunks - 1):
        receive_chunk(k)
        attend_all(blocks, 0, [chunk_at(k)], 3)
    project_edges()
    receive_chunk(ctx_chunks - 1)
    receive_halo()
    final = chunk_at(ctx_chunks - 1)

    part_blocks = rows // WINDOW_REACH

    def finish_part(slot):
        if early:
            edge = slot * (blocks - 1)
            from_block = slot * part_blocks + 1 - slot
            inside = [(from_block + i, [final]) for i in range(part_blocks - 1)]
            attend(inside + [(edge, [final, WINDOW])], last=True)

    if not early:
        attend_all(blocks, 0, [final, WINDOW], 2, last=True)
    loads[8].wait()
    out_tile = tile_of(width, 1024)

    def out_copy(d, mine):
        peer = lax.rem(tp + d, n_tp)
        slot = tp if mine else peer
        return pltpu.make_async_remote_copy(
            src_ref=partial_out.at[peer],
            dst_ref=partial_in.at[slot],
            send_sem=out_send.at[peer],
            recv_sem=out_recv.at[slot],
            device_id={"tp": peer},
            device_id_type=MESH,
        )

    def project_out(slot, store):
        source = pl.ds(pl.multiple_of(slot * rows, strip), rows)

        def one(j):
            cols = pl.ds(pl.multiple_of(j * out_tile, out_tile), out_tile)
            store(
                cols,
                jnp.dot(attended[source, :], wo[:, cols], preferred_element_type=F32).astype(BF16),
            )

        loop(0, width // out_tile, one)

    def peer_part(d):
        slot = lax.rem(tp + d, n_tp)
        finish_part(slot)

        def store(cols, value):
            partial_out[slot, :, cols] = value

        project_out(slot, store)
        out_copy(d, True).start()

    loop(1, n_tp, peer_part)
    finish_part(tp)

    def keep(cols, value):
        own_total[:, cols] = value.astype(F32)

    project_out(tp, keep)
    loop(1, n_tp, lambda d: out_copy(d, False).wait_recv())

    def finish(i):
        at = pl.ds(pl.multiple_of(i * strip, strip), strip)
        mixed = own_total[at, :]
        for d in range(1, n_tp):
            mixed = mixed + partial_in[lax.rem(tp + d, n_tp), at, :].astype(F32)
        out_ref[at, :] = (latent[at, :].astype(F32) + mod[4:5, :] * mixed).astype(BF16)

    loop(0, rows // strip, finish)

    loop(1, n_tp, lambda d: hid_copy(d, True).wait_send())
    loop(1, n_tp, lambda d: out_copy(d, True).wait_send())
    for copy in ctx_sends:
        copy.wait_send()

    if raw_halo:

        @pl.when(has_next & holds_last)
        def _():
            for piece in raw_pieces:
                raw_copy(True, piece).wait_send()

        @pl.when(has_last & holds_first)
        def _():
            for piece in raw_pieces:
                raw_copy(False, piece).wait_send()

        @pl.when(has_last & holds_last)
        def _():
            loop(1, n_tp, lambda d: edge_copy(True, d, True).wait_send())

        @pl.when(has_next & holds_first)
        def _():
            loop(1, n_tp, lambda d: edge_copy(False, d, True).wait_send())
    else:

        @pl.when(has_next)
        def _():
            for copy in halo_copies(True):
                copy.wait_send()

        @pl.when(has_last)
        def _():
            for copy in halo_copies(False):
                copy.wait_send()


def angle_tables(total_rows):
    inv_freq = np.power(
        10000.0, -np.arange(0, HEAD_DIM // 2, 2, dtype=np.float64) / (HEAD_DIM // 2)
    ).astype(np.float32)

    def tables(count):
        angle = (np.arange(count, dtype=np.float32)[:, None] * inv_freq).astype(np.float64)
        cosine, sine = np.cos(angle), np.sin(angle)
        return (
            np.concatenate([cosine, cosine], axis=1).astype(np.float32),
            np.concatenate([-sine, sine], axis=1).astype(np.float32),
        )

    empty = HEAD_DIM // 2
    by_row = [np.pad(t, ((0, 0), (0, empty))) for t in tables(total_rows // GRID_W)]
    by_col = [np.pad(t, ((0, 0), (empty, 0))) for t in tables(GRID_W)]
    return by_row + by_col


def shards(
    n_sp,
    n_tp,
    latent,
    condition,
    context_condition,
    context,
    norm_gain,
    shift_weight,
    scale_weight,
    gate_weight,
    query_weight,
    key_matrix,
    value_matrix,
    sink_logit_head,
    out_weight,
):
    rows, width = latent.shape
    group_rows = rows * n_tp
    angles = [jnp.asarray(t) for t in angle_tables(group_rows * n_sp)]
    columns = shift_weight.shape[1]
    groups = -(-5 * columns // LANES // 8) * 8
    query_width = query_weight.shape[1]
    pair = key_matrix.shape[1]
    ctx_rows = context.shape[0]
    lines = n_sp // QUAD
    ctx_sends = (lines - 1) + 4 * lines
    padded = group_rows + 2 * WINDOW_REACH
    state = (group_rows // WINDOW_REACH, pair // HEAD_DIM)
    stacked = query_width // pair * WINDOW_REACH
    dma = pltpu.SemaphoreType.DMA
    vmem = pl.BlockSpec(memory_space=pltpu.VMEM)
    anywhere = pl.BlockSpec(memory_space=pl.ANY)

    def like(array):
        return pltpu.VMEM(array.shape, array.dtype)

    return pl.pallas_call(
        functools.partial(block_kernel, n_sp, n_tp),
        out_shape=jax.ShapeDtypeStruct((rows, width), BF16),
        in_specs=[vmem] * 7 + [pl.BlockSpec(memory_space=pltpu.SMEM)] + [anywhere] * 9,
        out_specs=vmem,
        scratch_shapes=[
            like(latent),
            like(context),
            like(shift_weight),
            like(scale_weight),
            like(gate_weight),
            like(query_weight),
            like(key_matrix),
            like(value_matrix),
            like(out_weight),
            pltpu.VMEM((groups, LANES), F32),
            pltpu.VMEM((lines, groups, LANES), F32),
            pltpu.VMEM((n_tp, QUAD, groups, LANES), F32),
            pltpu.VMEM((8, width), F32),
            pltpu.VMEM((padded, width), BF16),
            like(context),
            pltpu.VMEM((group_rows, query_width), BF16),
            pltpu.VMEM((padded, pair), BF16),
            pltpu.VMEM((8 if rows % WINDOW_REACH == 0 else padded, pair), BF16),
            pltpu.VMEM((pair, padded), BF16),
            pltpu.VMEM((n_sp, ctx_rows, 2 * pair), BF16),
            pltpu.VMEM((pair, n_sp * ctx_rows), BF16),
            pltpu.VMEM((*state, HEAD_DIM + 8, stacked), F32),
            pltpu.VMEM((*state, 8, stacked), F32),
            pltpu.VMEM((group_rows, query_width), BF16),
            pltpu.VMEM((n_tp, rows, width), BF16),
            pltpu.VMEM((n_tp, rows, width), BF16),
            pltpu.VMEM((rows, width), F32),
            pltpu.VMEM((group_rows + 2 * WINDOW_REACH, HEAD_DIM), F32),
            pltpu.VMEM((group_rows + 2 * WINDOW_REACH, HEAD_DIM), F32),
            pltpu.VMEM((2, WINDOW_REACH, width), BF16),
            pltpu.VMEM((2 * WINDOW_REACH, width), BF16),
            dma((9,)),
            dma((lines,)),
            dma((lines,)),
            dma((n_tp, QUAD)),
            dma((n_tp, QUAD)),
            dma((n_tp,)),
            dma((n_tp,)),
            dma((ctx_sends,)),
            dma((n_sp, 2)),
            dma((2, 3)),
            dma((2, 3)),
            dma((2, n_tp)),
            dma((2,)),
            dma((n_tp,)),
            dma((n_tp,)),
        ],
        compiler_params=pltpu.CompilerParams(
            collective_id=0, has_side_effects=True, vmem_limit_bytes=63 * 1024 * 1024
        ),
    )(
        condition.reshape(1, -1),
        context_condition.reshape(1, -1),
        norm_gain.reshape(1, -1),
        *angles,
        sink_logit_head.reshape(1, -1),
        latent,
        context,
        shift_weight,
        scale_weight,
        gate_weight,
        query_weight,
        key_matrix,
        value_matrix,
        out_weight,
    )


def solution(mesh):
    placed = (
        P(("sp", "tp"), None),
        P("sp"),
        P("sp"),
        P("sp", None),
        P(),
        P("sp", "tp"),
        P("sp", "tp"),
        P("sp", "tp"),
        P(None, "tp"),
        P(None, "tp"),
        P(None, "tp"),
        P("tp"),
        P("tp", None),
    )
    return jax.shard_map(
        functools.partial(shards, mesh.shape["sp"], mesh.shape["tp"]),
        mesh=mesh,
        in_specs=placed,
        out_specs=P(("sp", "tp"), None),
        check_vma=False,
    )
```

```python
import functools

import jax
import jax.numpy as jnp
import numpy as np
from jax import lax
from jax.experimental import pallas as pl
from jax.experimental.pallas import tpu as pltpu
from jax.sharding import PartitionSpec as P

QUERY_HEADS = 16
KEY_VALUE_HEADS = 8
HEAD_DIM = 128
WINDOW_REACH = 128
GRID_W = 64
NORM_EPS = 1e-05
MASKED_SCORE = -1e30
LANES = 128
QUAD = 4
MESH = pl.DeviceIdType.MESH
F32 = jnp.float32
BF16 = jnp.bfloat16


def tile_of(extent, most):
    tile = min(extent, most)
    while extent % tile:
        tile -= LANES
    return tile


def block_kernel(
    n_sp,
    n_tp,
    cond_ref,
    ctx_cond_ref,
    gain_ref,
    row_cos,
    row_sin,
    col_cos,
    col_sin,
    sink_ref,
    latent_hbm,
    context_hbm,
    shift_hbm,
    scale_hbm,
    gate_hbm,
    wq_hbm,
    wk_hbm,
    wv_hbm,
    wo_hbm,
    out_ref,
    latent,
    context,
    shift_w,
    scale_w,
    gate_w,
    wq,
    wk,
    wv,
    wo,
    part,
    line_parts,
    quad_parts,
    mod,
    hidden,
    ctx_hidden,
    queries,
    keys_kept,
    values_kept,
    values_t,
    ctx_kv,
    ctx_values_t,
    sums,
    tops,
    attended,
    partial_out,
    partial_in,
    own_total,
    cos_ref,
    sin_ref,
    halo_raw,
    edge_hidden,
    load_sem,
    line_send,
    line_recv,
    quad_send,
    quad_recv,
    hid_send,
    hid_recv,
    ctx_send,
    ctx_recv,
    halo_send,
    halo_recv,
    edge_send,
    edge_recv,
    out_send,
    out_recv,
):
    sp = lax.axis_index("sp")
    tp = lax.axis_index("tp")
    rows, width = latent.shape
    group_rows = rows * n_tp
    columns = shift_w.shape[1]
    chunks = columns // LANES
    query_width = wq.shape[1]
    pair = wk.shape[1]
    kv_local = pair // HEAD_DIM
    per_group = query_width // pair
    ctx_rows = context.shape[0]

    loads = [
        pltpu.make_async_copy(src, dst, load_sem.at[i])
        for i, (src, dst) in enumerate(
            [
                (shift_hbm, shift_w),
                (scale_hbm, scale_w),
                (gate_hbm, gate_w),
                (context_hbm, context),
                (latent_hbm, latent),
                (wk_hbm, wk),
                (wv_hbm, wv),
                (wq_hbm, wq),
                (wo_hbm, wo),
            ]
        )
    ]
    for load in loads:
        load.start()

    barrier = pltpu.get_barrier_semaphore()

    lines = n_sp // QUAD
    line, corner = sp // QUAD, lax.rem(sp, QUAD)
    cluster = QUAD * n_tp

    def loop(low, high, f):
        def step(i, carry):
            f(i)
            return carry

        lax.fori_loop(low, high, step, 0)

    def in_line(d):
        peer = lax.rem(line + d, lines)
        return peer, {"sp": peer * QUAD + corner}

    def in_cluster(d):
        at = lax.rem(corner * n_tp + tp + d, cluster)
        peer, peer_tp = at // n_tp, lax.rem(at, n_tp)
        return peer, peer_tp, {"sp": line * QUAD + peer, "tp": peer_tp}

    def greet(device):
        pl.semaphore_signal(barrier, inc=1, device_id=device, device_id_type=MESH)

    loop(1, lines, lambda d: greet(in_line(d)[1]))
    loop(1, cluster, lambda d: greet(in_cluster(d)[2]))
    for d in (1, n_sp - 1):
        greet({"sp": lax.rem(sp + d, n_sp)})

    def silu(v):
        return v / (1.0 + jnp.exp(-v))

    depth = cond_ref.shape[1]
    row_id = lax.broadcasted_iota(jnp.int32, (16, depth), 0)
    active = jnp.where(
        row_id == 0,
        jnp.broadcast_to(silu(cond_ref[...]), (16, depth)),
        jnp.broadcast_to(silu(ctx_cond_ref[...]), (16, depth)),
    ).astype(BF16)
    part[...] = jnp.zeros_like(part)
    vector = 0
    for load, weight, count in zip(loads[:3], (shift_w, scale_w, gate_w), (2, 2, 1)):
        load.wait()
        product = jnp.dot(active, weight[...], preferred_element_type=F32)
        for v in range(count):
            for j in range(chunks):
                g = vector * chunks + j
                part[g : g + 1, :] = product[
                    v : v + 1, j * LANES : (j + 1) * LANES
                ]
            vector += 1

    pl.semaphore_wait(barrier, lines + cluster)

    def line_copy(d, mine):
        peer, device = in_line(d)
        slot = line if mine else peer
        return pltpu.make_async_remote_copy(
            src_ref=part,
            dst_ref=line_parts.at[slot],
            send_sem=line_send.at[peer],
            recv_sem=line_recv.at[slot],
            device_id=device,
            device_id_type=MESH,
        )

    has_next, has_last = sp < n_sp - 1, sp > 0
    holds_last, holds_first = tp == n_tp - 1, tp == 0
    raw_halo = rows >= WINDOW_REACH
    raw_ends = (0, 0, 128, 128)

    def raw_copy(up, piece):
        which = 0 if up else 1
        base = rows - WINDOW_REACH if up else 0
        begin, count = raw_ends[piece], raw_ends[piece + 1] - raw_ends[piece]
        return pltpu.make_async_remote_copy(
            src_ref=latent.at[pl.ds(base + begin, count)],
            dst_ref=halo_raw.at[which, pl.ds(begin, count)],
            send_sem=halo_send.at[which, piece],
            recv_sem=halo_recv.at[which, piece],
            device_id={"sp": lax.rem(sp + (1 if up else n_sp - 1), n_sp)},
            device_id_type=MESH,
        )

    raw_pieces = [i for i in range(3) if raw_ends[i + 1] > raw_ends[i]]

    def send_raw(piece):
        if raw_halo and piece in raw_pieces:

            @pl.when(has_next & holds_last)
            def _():
                raw_copy(True, piece).start()

            @pl.when(has_last & holds_first)
            def _():
                raw_copy(False, piece).start()

    loop(1, lines, lambda d: line_copy(d, True).start())
    line_parts[line] = part[...]
    loads[4].wait()
    loop(1, lines, lambda d: line_copy(d, True).wait_send())
    send_raw(0)

    strip = 32

    def scale_strip(i):
        at = pl.multiple_of(i * strip, strip)
        floats = latent[pl.ds(at, strip), :].astype(F32)
        inverse = lax.rsqrt(jnp.mean(floats * floats, axis=-1, keepdims=True) + NORM_EPS)
        own_total[pl.ds(at, strip), :] = floats * inverse

    loop(0, rows // strip, scale_strip)

    grid_rows = group_rows // GRID_W
    grid_pad = WINDOW_REACH // GRID_W
    in_row = lax.broadcasted_iota(jnp.int32, (GRID_W, HEAD_DIM), 1) < HEAD_DIM // 2

    def fill_angles(i):
        row = jnp.clip(sp * grid_rows - grid_pad + i, 0, n_sp * grid_rows - 1)
        at = pl.ds(pl.multiple_of(i * GRID_W, GRID_W), GRID_W)
        for target, by_row, by_col in ((cos_ref, row_cos, col_cos), (sin_ref, row_sin, col_sin)):
            spread = jnp.broadcast_to(by_row[pl.ds(row, 1), :], (GRID_W, HEAD_DIM))
            target[at, :] = jnp.where(in_row, spread, by_col[...])

    loop(0, grid_rows + 2 * grid_pad, fill_angles)
    loop(1, lines, lambda d: line_copy(d, False).wait_recv())
    quad_parts[tp, corner] = jnp.sum(line_parts[...], axis=0)

    def quad_copy(d, mine):
        peer, peer_tp, device = in_cluster(d)
        at = (tp, corner) if mine else (peer_tp, peer)
        return pltpu.make_async_remote_copy(
            src_ref=quad_parts.at[tp, corner],
            dst_ref=quad_parts.at[at],
            send_sem=quad_send.at[peer_tp, peer],
            recv_sem=quad_recv.at[at],
            device_id=device,
            device_id_type=MESH,
        )

    loop(1, cluster, lambda d: quad_copy(d, True).start())
    loop(1, cluster, lambda d: quad_copy(d, True).wait_send())
    send_raw(1)
    loop(1, cluster, lambda d: quad_copy(d, False).wait_recv())
    for t in range(n_tp):
        whole = jnp.sum(quad_parts[t], axis=0)
        for v in range(5):
            for j in range(chunks):
                g = v * chunks + j
                column = t * columns + j * LANES
                mod[v : v + 1, column : column + LANES] = whole[g : g + 1, :]
    gain = gain_ref[...]
    mod[2:3, :] = gain * (1.0 + mod[2:3, :])
    mod[3:4, :] = gain * (1.0 + mod[3:4, :])

    def normed(block, shift_row, scale_row):
        floats = block.astype(F32)
        inverse = lax.rsqrt(jnp.mean(floats * floats, axis=-1, keepdims=True) + NORM_EPS)
        return (
            floats * inverse * mod[scale_row : scale_row + 1, :] + mod[shift_row : shift_row + 1, :]
        ).astype(BF16)

    for i in (3, 5, 6):
        loads[i].wait()
    ctx_hidden[...] = normed(context[...], 1, 3)
    tile = tile_of(pair, 512)

    def ctx_project(j):
        at = pl.multiple_of(j * tile, tile)
        ctx_kv[sp, :, pl.ds(at, tile)] = jnp.dot(
            ctx_hidden[...], wk[:, pl.ds(at, tile)], preferred_element_type=F32
        ).astype(BF16)
        ctx_kv[sp, :, pl.ds(pl.multiple_of(pair + at, tile), tile)] = jnp.dot(
            ctx_hidden[...], wv[:, pl.ds(at, tile)], preferred_element_type=F32
        ).astype(BF16)

    loop(0, pair // tile, ctx_project)

    across = corner + 1 - 2 * lax.rem(corner, 2)
    beside = lax.rem(corner + 2, QUAD)
    opposite = QUAD - 1 - corner

    def ctx_copy(slot, peer, sem, half=None):
        cols = slice(None) if half is None else pl.ds(half * pair, pair)
        return pltpu.make_async_remote_copy(
            src_ref=ctx_kv.at[slot, :, cols],
            dst_ref=ctx_kv.at[slot, :, cols],
            send_sem=ctx_send.at[sem],
            recv_sem=ctx_recv.at[slot, half or 0],
            device_id={"sp": peer},
            device_id_type=MESH,
        )

    ctx_sends = []

    def send_ctx(slot, peer, half=None):
        copy = ctx_copy(slot, peer, len(ctx_sends), half)
        copy.start()
        ctx_sends.append(copy)

    def send_quad(slot):
        send_ctx(slot, line * QUAD + across)
        send_ctx(slot, line * QUAD + beside)

    for d in range(1, lines):
        send_ctx(sp, lax.rem(line + d, lines) * QUAD + corner)
    send_quad(sp)
    send_raw(2)

    def line_base(d):
        return lax.rem(line + lines - d, lines) * QUAD

    def forward(d):
        slot = line_base(d) + corner
        ctx_copy(slot, sp, 0).wait_recv()
        send_quad(slot)

    def relay(d):
        ctx_copy(line_base(d) + across, sp, 0).wait_recv()
        send_ctx(line_base(d) + across, line * QUAD + beside, 0)
        ctx_copy(line_base(d) + beside, sp, 0).wait_recv()
        send_ctx(line_base(d) + beside, line * QUAD + across, 1)

    gather_steps = []
    for d in range(lines):
        if d + 1 < lines:
            gather_steps.append(functools.partial(forward, d + 1))
        gather_steps.append(functools.partial(relay, d))

    def serve(count):
        for step in gather_steps[:count]:
            step()
        del gather_steps[:count]

    own_start = pl.multiple_of(WINDOW_REACH + tp * rows, strip)

    def norm_strip(i):
        at = pl.multiple_of(i * strip, strip)
        hidden[pl.ds(pl.multiple_of(own_start + at, strip), strip), :] = (
            own_total[pl.ds(at, strip), :] * mod[2:3, :] + mod[0:1, :]
        ).astype(BF16)

    loop(0, rows // strip, norm_strip)

    def hid_copy(d, mine):
        peer = lax.rem(tp + d, n_tp)
        slot = tp if mine else peer
        at = pl.multiple_of(WINDOW_REACH + slot * rows, strip)
        mine_at = pl.multiple_of(WINDOW_REACH + tp * rows, strip)
        return pltpu.make_async_remote_copy(
            src_ref=hidden.at[pl.ds(mine_at, rows)],
            dst_ref=hidden.at[pl.ds(at, rows)],
            send_sem=hid_send.at[peer],
            recv_sem=hid_recv.at[slot],
            device_id={"tp": peer},
            device_id_type=MESH,
        )

    loop(1, n_tp, lambda d: hid_copy(d, True).start())

    quarter = HEAD_DIM // 4
    def turned(values, cosine, sine):
        pieces = []
        lane = lax.broadcasted_iota(jnp.int32, cosine.shape, 1)
        low_half = lax.rem(lane, 2 * quarter) < quarter
        for h in range(values.shape[1] // HEAD_DIM):
            u = values[:, h * HEAD_DIM : (h + 1) * HEAD_DIM]
            other = jnp.where(
                low_half, pltpu.roll(u, HEAD_DIM - quarter, 1), pltpu.roll(u, quarter, 1)
            )
            pieces.append(u * cosine + other * sine)
        return jnp.concatenate(pieces, axis=1).astype(BF16)

    aligned = rows % WINDOW_REACH == 0

    def project_kv(start):
        source = pl.ds(pl.multiple_of(start, strip), rows)

        def one(j):
            col = pl.multiple_of(j * tile, tile)
            keys = jnp.dot(hidden[source, :], wk[:, pl.ds(col, tile)], preferred_element_type=F32)
            keys_kept[source, pl.ds(col, tile)] = turned(keys, cos_ref[source, :], sin_ref[source, :])
            values = jnp.dot(hidden[source, :], wv[:, pl.ds(col, tile)], preferred_element_type=F32)
            if aligned:
                at = pl.ds(pl.multiple_of(start, WINDOW_REACH), rows)
                values_t[pl.ds(col, tile), at] = values.astype(BF16).T
            else:
                values_kept[source, pl.ds(col, tile)] = values.astype(BF16)

        loop(0, pair // tile, one)

    def transpose_values():
        if not aligned:

            def one(i):
                at = pl.ds(pl.multiple_of(WINDOW_REACH * (i + 1), WINDOW_REACH), WINDOW_REACH)
                values_t[:, at] = values_kept[at, :].T

            loop(0, group_rows // WINDOW_REACH, one)

    def project_q(slot, begin=0, end=None):
        target = pl.ds(pl.multiple_of(slot * rows, strip), rows)
        source = pl.ds(pl.multiple_of(WINDOW_REACH + slot * rows, strip), rows)
        q_tile = tile_of(query_width, 512)

        def one(j):
            col = pl.multiple_of(j * q_tile, q_tile)
            q = jnp.dot(hidden[source, :], wq[:, pl.ds(col, q_tile)], preferred_element_type=F32)
            queries[target, pl.ds(col, q_tile)] = turned(
                q * factor, cos_ref[source, :], sin_ref[source, :]
            )

        count = query_width // q_tile
        loop(begin * count // 2, (2 if end is None else end) * count // 2, one)

    log2e = 1.4426950408889634
    factor = HEAD_DIM ** (-0.5) * log2e
    def halo_copies(up):
        source = group_rows if up else WINDOW_REACH
        target = 0 if up else group_rows + WINDOW_REACH
        which = 0 if up else 1
        peer = {"sp": lax.rem(sp + (1 if up else n_sp - 1), n_sp)}
        ends = (
            (keys_kept.at[pl.ds(source, WINDOW_REACH)], keys_kept.at[pl.ds(target, WINDOW_REACH)]),
            (
                values_t.at[:, pl.ds(source, WINDOW_REACH)],
                values_t.at[:, pl.ds(target, WINDOW_REACH)],
            ),
        )
        return [
            pltpu.make_async_remote_copy(
                src_ref=src,
                dst_ref=dst,
                send_sem=halo_send.at[which, i],
                recv_sem=halo_recv.at[which, i],
                device_id=peer,
                device_id_type=MESH,
            )
            for i, (src, dst) in enumerate(ends)
        ]

    def send_halo():
        if raw_halo:
            return

        @pl.when(has_next)
        def _():
            for copy in halo_copies(True):
                copy.start()

        @pl.when(has_last)
        def _():
            for copy in halo_copies(False):
                copy.start()

        def clear(at):
            region = pl.ds(at, WINDOW_REACH)
            keys_kept[region, :] = jnp.zeros((WINDOW_REACH, pair), BF16)
            values_t[:, region] = jnp.zeros((pair, WINDOW_REACH), BF16)

        @pl.when(jnp.logical_not(has_last))
        def _():
            clear(0)

        @pl.when(jnp.logical_not(has_next))
        def _():
            clear(group_rows + WINDOW_REACH)

    def edge_copy(low, d, mine):
        peer = lax.rem(tp + d, n_tp) if mine else tp
        which = 0 if low else 1
        region = pl.ds(which * WINDOW_REACH, WINDOW_REACH)
        return pltpu.make_async_remote_copy(
            src_ref=edge_hidden.at[region],
            dst_ref=edge_hidden.at[region],
            send_sem=edge_send.at[which, peer],
            recv_sem=edge_recv.at[which],
            device_id={"tp": peer},
            device_id_type=MESH,
        )

    def scale_edge(low):
        which = 0 if low else 1
        for piece in raw_pieces:
            raw_copy(low, piece).wait_recv()

        def one(i):
            at = pl.multiple_of(i * strip, strip)
            edge_hidden[pl.ds(which * WINDOW_REACH + at, strip), :] = normed(
                halo_raw[which, pl.ds(at, strip), :], 0, 2
            )

        loop(0, WINDOW_REACH // strip, one)
        loop(1, n_tp, lambda d: edge_copy(low, d, True).start())

    def scale_edges():
        if not raw_halo:
            return

        @pl.when(has_last & holds_last)
        def _():
            scale_edge(True)

        @pl.when(has_next & holds_first)
        def _():
            scale_edge(False)

        @pl.when(jnp.logical_not(has_last))
        def _():
            edge_hidden[:WINDOW_REACH, :] = jnp.zeros((WINDOW_REACH, width), BF16)

        @pl.when(jnp.logical_not(has_next))
        def _():
            edge_hidden[WINDOW_REACH:, :] = jnp.zeros((WINDOW_REACH, width), BF16)

    def project_edges():
        if not raw_halo:
            return

        @pl.when(has_last & jnp.logical_not(holds_last))
        def _():
            edge_copy(True, 0, False).wait_recv()

        @pl.when(has_next & jnp.logical_not(holds_first))
        def _():
            edge_copy(False, 0, False).wait_recv()

        def one(j):
            col = pl.multiple_of(j * tile, tile)
            keys = jnp.dot(edge_hidden[...], wk[:, pl.ds(col, tile)], preferred_element_type=F32)
            values = jnp.dot(edge_hidden[...], wv[:, pl.ds(col, tile)], preferred_element_type=F32)
            for which, start in enumerate((0, WINDOW_REACH + group_rows)):
                part = slice(which * WINDOW_REACH, (which + 1) * WINDOW_REACH)
                at = pl.ds(start, WINDOW_REACH)
                keys_kept[at, pl.ds(col, tile)] = turned(keys[part], cos_ref[at, :], sin_ref[at, :])
                values_t[pl.ds(col, tile), at] = values[part].astype(BF16).T

        loop(0, pair // tile, one)

    def receive_halo():
        if raw_halo:
            return

        @pl.when(has_last)
        def _():
            for copy in halo_copies(True):
                copy.wait_recv()

        @pl.when(has_next)
        def _():
            for copy in halo_copies(False):
                copy.wait_recv()

    span = 3 * WINDOW_REACH
    stacked = per_group * WINDOW_REACH
    contract = (((1,), (1,)), ((), ()))
    blocks = group_rows // WINDOW_REACH
    lines_each = max(1, 256 // (QUAD * ctx_rows))
    ctx_chunks = lines // lines_each
    slots_each = QUAD * lines_each
    chunk_rows = slots_each * ctx_rows
    ahead = lax.rem(
        lax.broadcasted_iota(jnp.int32, (WINDOW_REACH, stacked), 1), WINDOW_REACH
    ) - lax.broadcasted_iota(jnp.int32, (WINDOW_REACH, stacked), 0)
    WINDOW = "window"

    def chunk_at(k):
        return lax.rem(line // lines_each + ctx_chunks - k, ctx_chunks)

    def query_heads(h):
        return range(h * per_group, (h + 1) * per_group)

    def scores(block, h, piece):
        begin = pl.multiple_of(block * WINDOW_REACH, WINDOW_REACH)
        cols = slice(h * HEAD_DIM, (h + 1) * HEAD_DIM)
        q = jnp.concatenate(
            [
                queries[pl.ds(begin, WINDOW_REACH), i * HEAD_DIM : (i + 1) * HEAD_DIM]
                for i in query_heads(h)
            ],
            axis=0,
        )
        if piece is not WINDOW:
            keys = ctx_kv[pl.ds(piece * slots_each, slots_each), :, cols]
            keys = keys.reshape(chunk_rows, HEAD_DIM)
            return lax.dot_general(keys, q, contract, preferred_element_type=F32)
        keys = keys_kept[pl.ds(begin, span), cols]
        band = lax.dot_general(keys, q, contract, preferred_element_type=F32)
        lowest = jnp.where((block > 0) | has_last, 0, -span)
        highest = jnp.where((block < blocks - 1) | has_next, 0, span)
        return jnp.concatenate(
            [
                jnp.where(ahead <= lowest, band[:WINDOW_REACH], MASKED_SCORE),
                band[WINDOW_REACH : 2 * WINDOW_REACH],
                jnp.where(ahead >= highest, band[2 * WINDOW_REACH :], MASKED_SCORE),
            ],
            axis=0,
        )

    def weighted(block, h, piece, probs):
        cols = slice(h * HEAD_DIM, (h + 1) * HEAD_DIM)
        if piece is WINDOW:
            begin = pl.multiple_of(block * WINDOW_REACH, WINDOW_REACH)
            values = values_t[cols, pl.ds(begin, span)]
        else:
            begin = pl.multiple_of(piece * chunk_rows, chunk_rows)
            values = ctx_values_t[cols, pl.ds(begin, chunk_rows)]
        ones = jnp.ones((16, probs.shape[0]), BF16)
        return jnp.dot(
            jnp.concatenate([values, ones], axis=0), probs, preferred_element_type=F32
        )[: HEAD_DIM + 8]

    def sinks(h):
        return jnp.concatenate(
            [jnp.full((1, WINDOW_REACH), sink_ref[0, i] * log2e, F32) for i in query_heads(h)],
            axis=1,
        )

    def attend(items, first=False, last=False):
        tasks = [(b, h, pieces) for b, pieces in items for h in range(kv_local)]
        top, total = {}, {}
        following = {i: scores(b, h, pieces[0]) for i, (b, h, pieces) in enumerate(tasks)}
        for step in range(max(len(pieces) for _, pieces in items)):
            current, following, now = following, {}, {}
            live = [(i, *task) for i, task in enumerate(tasks) if step < len(task[2])]
            for i, b, h, pieces in live:
                if step + 1 < len(pieces):
                    following[i] = scores(b, h, pieces[step + 1])
            for i, b, h, pieces in live:
                if step == 0:
                    top[i] = sinks(h) if first else tops[b, h, 0:1, :]
                now[i] = jnp.maximum(top[i], jnp.max(current[i], axis=0, keepdims=True))
            probs = {i: jnp.exp2(current[i] - now[i]).astype(BF16) for i, *_ in live}
            for i, b, h, pieces in live:
                added = weighted(b, h, pieces[step], probs[i])
                shrink = jnp.exp2(top[i] - now[i])
                if step == 0 and first:
                    total[i] = jnp.concatenate(
                        [added[:HEAD_DIM], added[HEAD_DIM:] + shrink], axis=0
                    )
                else:
                    total[i] = (sums[b, h] if step == 0 else total[i]) * shrink + added
                top[i] = now[i]
        for i, (b, h, pieces) in enumerate(tasks):
            if last:
                mixed = total[i][:HEAD_DIM] / total[i][HEAD_DIM : HEAD_DIM + 1]
                mixed = mixed.T.astype(BF16)
                here = pl.ds(pl.multiple_of(b * WINDOW_REACH, WINDOW_REACH), WINDOW_REACH)
                for n, k in enumerate(query_heads(h)):
                    attended[here, k * HEAD_DIM : (k + 1) * HEAD_DIM] = mixed[
                        n * WINDOW_REACH : (n + 1) * WINDOW_REACH
                    ]
            else:
                sums[b, h] = total[i]
                tops[b, h, 0:1, :] = top[i]

    def attend_all(n, first_block, pieces, most, **kind):
        each = max(i for i in range(1, most + 1) if n % i == 0)
        loop(
            0,
            n // each,
            lambda g: attend([(first_block + g * each + i, pieces) for i in range(each)], **kind),
        )

    def start_block(b):
        for h in range(kv_local):
            sums[b, h, :HEAD_DIM, :] = jnp.zeros((HEAD_DIM, stacked), F32)
            sums[b, h, HEAD_DIM:, :] = jnp.ones((8, stacked), F32)
            tops[b, h, 0:1, :] = sinks(h)

    def opposite_arrived(base):
        for half in range(2):
            ctx_copy(base + opposite, sp, 0, half).wait_recv()

    def transpose_chunk(piece):
        values = ctx_kv[pl.ds(piece * slots_each, slots_each), :, pl.ds(pair, pair)]
        at = pl.multiple_of(piece * chunk_rows, chunk_rows)
        ctx_values_t[:, pl.ds(at, chunk_rows)] = values.reshape(chunk_rows, pair).T

    def receive_chunk(k):
        if lines_each == 1:
            opposite_arrived(line_base(k))
        elif k == 0:
            loop(0, lines, lambda i: opposite_arrived(i * QUAD))
        transpose_chunk(chunk_at(k))

    early = aligned and n_tp == 2 and blocks >= 6
    inner = blocks - 2

    loads[7].wait()
    project_kv(WINDOW_REACH + tp * rows)
    project_q(tp)
    loop(1, n_tp, lambda d: hid_copy(d, False).wait_recv())
    serve(2)
    loop(1, n_tp, lambda d: project_kv(WINDOW_REACH + lax.rem(tp + d, n_tp) * rows))
    transpose_values()
    send_halo()
    if early:
        project_q(1 - tp, 0, 1)
        serve(1)
        project_q(1 - tp, 1, 2)
        serve(1)
        attend_all(inner, 1, [WINDOW], 2, first=True)
        start_block(0)
        start_block(blocks - 1)
        scale_edges()
        serve(2)
    else:
        loop(1, n_tp, lambda d: project_q(lax.rem(tp + d, n_tp)))
        loop(0, blocks, start_block)
        scale_edges()
    if lines_each > 1:
        serve(len(gather_steps))
    receive_chunk(0)
    attend_all(blocks, 0, [chunk_at(0)], 3)
    project_edges()
    serve(len(gather_steps))
    for k in range(1, ctx_chunks - 1):
        receive_chunk(k)
        attend_all(blocks, 0, [chunk_at(k)], 3)
    receive_chunk(ctx_chunks - 1)
    receive_halo()
    final = chunk_at(ctx_chunks - 1)

    part_blocks = rows // WINDOW_REACH

    def finish_part(slot):
        if early:
            edge = slot * (blocks - 1)
            from_block = slot * part_blocks + 1 - slot
            inside = [(from_block + i, [final]) for i in range(part_blocks - 1)]
            attend(inside + [(edge, [final, WINDOW])], last=True)

    if not early:
        attend_all(blocks, 0, [final, WINDOW], 2, last=True)
    loads[8].wait()
    out_tile = tile_of(width, 1024)

    def out_copy(d, mine):
        peer = lax.rem(tp + d, n_tp)
        slot = tp if mine else peer
        return pltpu.make_async_remote_copy(
            src_ref=partial_out.at[peer],
            dst_ref=partial_in.at[slot],
            send_sem=out_send.at[peer],
            recv_sem=out_recv.at[slot],
            device_id={"tp": peer},
            device_id_type=MESH,
        )

    def project_out(slot, store):
        source = pl.ds(pl.multiple_of(slot * rows, strip), rows)

        def one(j):
            cols = pl.ds(pl.multiple_of(j * out_tile, out_tile), out_tile)
            store(
                cols,
                jnp.dot(attended[source, :], wo[:, cols], preferred_element_type=F32).astype(BF16),
            )

        loop(0, width // out_tile, one)

    def peer_part(d):
        slot = lax.rem(tp + d, n_tp)
        finish_part(slot)

        def store(cols, value):
            partial_out[slot, :, cols] = value

        project_out(slot, store)
        out_copy(d, True).start()

    loop(1, n_tp, peer_part)
    finish_part(tp)

    def keep(cols, value):
        own_total[:, cols] = value.astype(F32)

    project_out(tp, keep)
    loop(1, n_tp, lambda d: out_copy(d, False).wait_recv())

    def finish(i):
        at = pl.ds(pl.multiple_of(i * strip, strip), strip)
        mixed = own_total[at, :]
        for d in range(1, n_tp):
            mixed = mixed + partial_in[lax.rem(tp + d, n_tp), at, :].astype(F32)
        out_ref[at, :] = (latent[at, :].astype(F32) + mod[4:5, :] * mixed).astype(BF16)

    loop(0, rows // strip, finish)

    loop(1, n_tp, lambda d: hid_copy(d, True).wait_send())
    loop(1, n_tp, lambda d: out_copy(d, True).wait_send())
    for copy in ctx_sends:
        copy.wait_send()

    if raw_halo:

        @pl.when(has_next & holds_last)
        def _():
            for piece in raw_pieces:
                raw_copy(True, piece).wait_send()

        @pl.when(has_last & holds_first)
        def _():
            for piece in raw_pieces:
                raw_copy(False, piece).wait_send()

        @pl.when(has_last & holds_last)
        def _():
            loop(1, n_tp, lambda d: edge_copy(True, d, True).wait_send())

        @pl.when(has_next & holds_first)
        def _():
            loop(1, n_tp, lambda d: edge_copy(False, d, True).wait_send())
    else:

        @pl.when(has_next)
        def _():
            for copy in halo_copies(True):
                copy.wait_send()

        @pl.when(has_last)
        def _():
            for copy in halo_copies(False):
                copy.wait_send()


def angle_tables(total_rows):
    inv_freq = np.power(
        10000.0, -np.arange(0, HEAD_DIM // 2, 2, dtype=np.float64) / (HEAD_DIM // 2)
    ).astype(np.float32)

    def tables(count):
        angle = (np.arange(count, dtype=np.float32)[:, None] * inv_freq).astype(np.float64)
        cosine, sine = np.cos(angle), np.sin(angle)
        return (
            np.concatenate([cosine, cosine], axis=1).astype(np.float32),
            np.concatenate([-sine, sine], axis=1).astype(np.float32),
        )

    empty = HEAD_DIM // 2
    by_row = [np.pad(t, ((0, 0), (0, empty))) for t in tables(total_rows // GRID_W)]
    by_col = [np.pad(t, ((0, 0), (empty, 0))) for t in tables(GRID_W)]
    return by_row + by_col


def shards(
    n_sp,
    n_tp,
    latent,
    condition,
    context_condition,
    context,
    norm_gain,
    shift_weight,
    scale_weight,
    gate_weight,
    query_weight,
    key_matrix,
    value_matrix,
    sink_logit_head,
    out_weight,
):
    rows, width = latent.shape
    group_rows = rows * n_tp
    angles = [jnp.asarray(t) for t in angle_tables(group_rows * n_sp)]
    columns = shift_weight.shape[1]
    groups = -(-5 * columns // LANES // 8) * 8
    query_width = query_weight.shape[1]
    pair = key_matrix.shape[1]
    ctx_rows = context.shape[0]
    lines = n_sp // QUAD
    ctx_sends = (lines - 1) + 4 * lines
    padded = group_rows + 2 * WINDOW_REACH
    state = (group_rows // WINDOW_REACH, pair // HEAD_DIM)
    stacked = query_width // pair * WINDOW_REACH
    dma = pltpu.SemaphoreType.DMA
    vmem = pl.BlockSpec(memory_space=pltpu.VMEM)
    anywhere = pl.BlockSpec(memory_space=pl.ANY)

    def like(array):
        return pltpu.VMEM(array.shape, array.dtype)

    return pl.pallas_call(
        functools.partial(block_kernel, n_sp, n_tp),
        out_shape=jax.ShapeDtypeStruct((rows, width), BF16),
        in_specs=[vmem] * 7 + [pl.BlockSpec(memory_space=pltpu.SMEM)] + [anywhere] * 9,
        out_specs=vmem,
        scratch_shapes=[
            like(latent),
            like(context),
            like(shift_weight),
            like(scale_weight),
            like(gate_weight),
            like(query_weight),
            like(key_matrix),
            like(value_matrix),
            like(out_weight),
            pltpu.VMEM((groups, LANES), F32),
            pltpu.VMEM((lines, groups, LANES), F32),
            pltpu.VMEM((n_tp, QUAD, groups, LANES), F32),
            pltpu.VMEM((8, width), F32),
            pltpu.VMEM((padded, width), BF16),
            like(context),
            pltpu.VMEM((group_rows, query_width), BF16),
            pltpu.VMEM((padded, pair), BF16),
            pltpu.VMEM((8 if rows % WINDOW_REACH == 0 else padded, pair), BF16),
            pltpu.VMEM((pair, padded), BF16),
            pltpu.VMEM((n_sp, ctx_rows, 2 * pair), BF16),
            pltpu.VMEM((pair, n_sp * ctx_rows), BF16),
            pltpu.VMEM((*state, HEAD_DIM + 8, stacked), F32),
            pltpu.VMEM((*state, 8, stacked), F32),
            pltpu.VMEM((group_rows, query_width), BF16),
            pltpu.VMEM((n_tp, rows, width), BF16),
            pltpu.VMEM((n_tp, rows, width), BF16),
            pltpu.VMEM((rows, width), F32),
            pltpu.VMEM((group_rows + 2 * WINDOW_REACH, HEAD_DIM), F32),
            pltpu.VMEM((group_rows + 2 * WINDOW_REACH, HEAD_DIM), F32),
            pltpu.VMEM((2, WINDOW_REACH, width), BF16),
            pltpu.VMEM((2 * WINDOW_REACH, width), BF16),
            dma((9,)),
            dma((lines,)),
            dma((lines,)),
            dma((n_tp, QUAD)),
            dma((n_tp, QUAD)),
            dma((n_tp,)),
            dma((n_tp,)),
            dma((ctx_sends,)),
            dma((n_sp, 2)),
            dma((2, 3)),
            dma((2, 3)),
            dma((2, n_tp)),
            dma((2,)),
            dma((n_tp,)),
            dma((n_tp,)),
        ],
        compiler_params=pltpu.CompilerParams(
            collective_id=0, has_side_effects=True, vmem_limit_bytes=63 * 1024 * 1024
        ),
    )(
        condition.reshape(1, -1),
        context_condition.reshape(1, -1),
        norm_gain.reshape(1, -1),
        *angles,
        sink_logit_head.reshape(1, -1),
        latent,
        context,
        shift_weight,
        scale_weight,
        gate_weight,
        query_weight,
        key_matrix,
        value_matrix,
        out_weight,
    )


def solution(mesh):
    placed = (
        P(("sp", "tp"), None),
        P("sp"),
        P("sp"),
        P("sp", None),
        P(),
        P("sp", "tp"),
        P("sp", "tp"),
        P("sp", "tp"),
        P(None, "tp"),
        P(None, "tp"),
        P(None, "tp"),
        P("tp"),
        P("tp", None),
    )
    return jax.shard_map(
        functools.partial(shards, mesh.shape["sp"], mesh.shape["tp"]),
        mesh=mesh,
        in_specs=placed,
        out_specs=P(("sp", "tp"), None),
        check_vma=False,
    )
```
